512 devices in a mesh: sp: 64 (over z, y), tp: 8 (over x, core).
Axes of the slice: x: 4, y: 4, z: 16, core: 2. Of those that a mesh axis runs over, the one named last changes fastest.
Arguments:
- stream: bfloat16 [16384, 2048], P(('sp', 'tp')), may hold values from -6 to 6
- queries: bfloat16 [16384, 1024], P('sp', 'tp'), may hold values from -6 to 6
- keys_in: bfloat16 [16384, 1024], P('sp', 'tp'), may hold values from -6 to 6
- values_in: bfloat16 [16384, 1024], P('sp', 'tp'), may hold values from -6 to 6
- gate_in: bfloat16 [16384, 1024], P('sp', 'tp'), may hold values from -6 to 6
- log_decay: float32 [16384, 8], P('sp', 'tp'), may hold values from -0.8 to 0
- head_gain: bfloat16 [1024], P('tp'), may hold values from 0.099609375 to 1.8984375
- out_weight: bfloat16 [1024, 2048], P('tp'), may hold values from -0.1875 to 0.1875
- norm_gain: bfloat16 [2048], replicated, may hold values from 0.099609375 to 1.8984375
- gate_weight: bfloat16 [2048, 5632], P('sp', 'tp'), may hold values from -0.125 to 0.125
- up_weight: bfloat16 [2048, 5632], P('sp', 'tp'), may hold values from -0.125 to 0.125
- down_weight: bfloat16 [5632, 2048], P('tp', 'sp'), may hold values from -0.078125 to 0.078125
Outputs:
- result: bfloat16 [16384, 2048], P(('sp', 'tp'))
The draws below stay inside these ranges and needn't reach their ends.
All inputs are finite; a program needn't handle non-finite values.
Results may differ from the reference program's by a relative error of at most 0.02.
Values may be sent and summed in bfloat16 or wider, within the bound.
No kernel may reach another device: no remote copies, remote signals or barrier semaphores. Data moves between devices by JAX's collectives and lax.ppermute only.
A program may use at most 64 MiB of HBM per device.

```python
import jax
import jax.numpy as jnp
from jax import lax

D = 2048
HEAD_COUNT = 8
HEAD_DIM = 128
FF = 5632
BLOCK = 128
TOK_DEV = 256
TOKEN_COUNT = 16384
N_TP = 8


def draw_log_decay(key, part):
    draw_keys = jax.random.split(jax.random.fold_in(key, 11), 7)
    is_fast = jax.random.randint(draw_keys[0], (HEAD_COUNT,), 0, 2) == 0
    slow_rate = jax.random.uniform(draw_keys[1], (HEAD_COUNT,), jnp.float32, 0.2, 0.6) / TOKEN_COUNT
    fast_rate = 1.0 / jax.random.uniform(draw_keys[2], (HEAD_COUNT,), jnp.float32, 30.0, 100.0)
    head_rate = jnp.where(is_fast, fast_rate, slow_rate)
    block_count = TOKEN_COUNT // TOK_DEV
    block_factor = jax.random.uniform(draw_keys[3], (block_count, 1, HEAD_COUNT), jnp.float32, 0.4, 1.6)
    roughness = jax.random.uniform(draw_keys[4], (block_count, TOK_DEV, HEAD_COUNT), jnp.float32, 0.5, 1.5)
    drawn_reference = -(head_rate * block_factor * roughness).reshape(TOKEN_COUNT, HEAD_COUNT)
    spike_locations = jax.random.randint(draw_keys[5], (2, HEAD_COUNT), 0, TOKEN_COUNT)
    spike_drops = jnp.log(jax.random.uniform(draw_keys[6], (2, HEAD_COUNT), jnp.float32, 0.5, 0.8))
    token_positions = jnp.arange(TOKEN_COUNT)[:, None]
    spike_events = jnp.sum(jnp.where(token_positions[None] == spike_locations[:, None, :], spike_drops[:, None, :], 0.0), axis=0)
    return drawn_reference + spike_events


def level_of(own_key, extent, cuts, smallest, largest):
    level = 1.0
    for position, blocks in cuts:
        heights = jax.random.uniform(jax.random.fold_in(jax.random.fold_in(own_key, 6), position), (blocks,), jnp.float32, smallest / len(cuts), largest / len(cuts))
        level = level * jnp.repeat(jnp.exp(heights), extent[position] // blocks).reshape((-1,) + (1,) * (len(extent) - 1 - position))
    return level


def centred(own_key, extent, scale, bound, cuts=(), held_as=jnp.bfloat16):
    drawn = scale * jax.random.normal(own_key, extent, jnp.float32)
    if cuts:
        drawn = drawn * level_of(own_key, extent, cuts, -0.22, 0.18)
    return jnp.clip(drawn, -bound, bound).astype(held_as)


def setup_inputs(seed: int = 0) -> dict:
    streams_of = jax.random.split(jax.random.key(seed), 13)
    return {
        "stream": centred(streams_of[0], (TOKEN_COUNT, D), 0.7, 6.0, ((0, 512),)),
        "queries": centred(streams_of[1], (TOKEN_COUNT, HEAD_COUNT * HEAD_DIM), 1.0, 6.0, ((0, 64), (1, 8))),
        "keys_in": centred(streams_of[2], (TOKEN_COUNT, HEAD_COUNT * HEAD_DIM), 1.0, 6.0, ((0, 64), (1, 8))),
        "values_in": centred(streams_of[3], (TOKEN_COUNT, HEAD_COUNT * HEAD_DIM), 1.0, 6.0, ((0, 64), (1, 8))),
        "gate_in": centred(streams_of[4], (TOKEN_COUNT, HEAD_COUNT * HEAD_DIM), 1.0, 6.0, ((0, 64), (1, 8))),
        "log_decay": draw_log_decay(jax.random.fold_in(streams_of[12], 71), 0),
        "head_gain": jnp.clip(1.0 + 0.18 * jax.random.normal(streams_of[6], (HEAD_COUNT * HEAD_DIM,), jnp.float32), 0.099609375, 1.8984375).astype(jnp.bfloat16),
        "out_weight": centred(streams_of[7], (HEAD_COUNT * HEAD_DIM, D), (HEAD_COUNT * HEAD_DIM) ** -0.5, 0.1875, ((0, 8),)),
        "norm_gain": jnp.clip(1.0 + 0.18 * jax.random.normal(streams_of[8], (D,), jnp.float32), 0.099609375, 1.8984375).astype(jnp.bfloat16),
        "gate_weight": centred(streams_of[9], (D, FF), D ** -0.5, 0.125, ((0, 64), (1, 8))),
        "up_weight": centred(streams_of[10], (D, FF), D ** -0.5, 0.125, ((0, 64), (1, 8))),
        "down_weight": centred(streams_of[11], (FF, D), FF ** -0.5, 0.078125, ((0, 8), (1, 64))),
    }


epsilon = 1e-06
highest = lax.Precision.HIGHEST

def block_pass(state, block_inputs):
    query_block, key_block, value_block, decay_block = block_inputs
    head_dim = query_block.shape[-1]
    key_scale = head_dim ** (-0.5)
    running = jnp.cumsum(decay_block, axis=0)
    query_wide = query_block.astype(jnp.float32)
    key_plain = key_block.astype(jnp.float32)
    value_wide = value_block.astype(jnp.float32)
    scores = jnp.einsum('ihd,jhd->hij', query_wide, key_plain, precision=highest) * key_scale
    offsets = jnp.arange(decay_block.shape[0])
    causal = offsets[:, None] >= offsets[None, :]
    log_gap = running.T[:, :, None] - running.T[:, None, :]
    decay_table = jnp.where(causal[None], jnp.exp(jnp.minimum(log_gap, 0.0)), 0.0)
    within = jnp.einsum('hij,jhe->ihe', scores * decay_table, value_wide, precision=highest)
    carried = jnp.einsum('ihd,hde->ihe', query_wide * jnp.exp(running)[:, :, None], state, precision=highest)
    block_total = running[-1]
    key_wide = key_plain * key_scale * jnp.exp(block_total[None] - running)[:, :, None]
    state = jnp.exp(block_total)[:, None, None] * state + jnp.einsum('jhd,jhe->hde', key_wide, value_wide, precision=highest)
    return (state, within + carried)

def reference(stream, queries, keys_in, values_in, gate_in, log_decay, head_gain, out_weight, norm_gain, gate_weight, up_weight, down_weight):
    heads = log_decay.shape[1]
    head_dim = queries.shape[1] // heads
    block_count = TOKEN_COUNT // BLOCK
    block_shape = (block_count, BLOCK, heads, head_dim)
    block_inputs = (queries.reshape(block_shape), keys_in.reshape(block_shape), values_in.reshape(block_shape), log_decay.reshape(block_count, BLOCK, heads))
    start_state = jnp.zeros((heads, head_dim, head_dim), jnp.float32)
    final_state, retained = lax.scan(block_pass, start_state, block_inputs)
    retained = retained.reshape(TOKEN_COUNT, heads, head_dim)
    center = lax.optimization_barrier(jnp.mean(retained, axis=-1, keepdims=True))
    spread = lax.optimization_barrier(jnp.mean(jnp.square(retained - center), axis=-1, keepdims=True))
    normed_heads = (retained - center) * lax.rsqrt(spread + epsilon) * head_gain.astype(jnp.float32).reshape(heads, head_dim)
    mixed = (jax.nn.silu(gate_in.astype(jnp.float32)) * normed_heads.reshape(TOKEN_COUNT, heads * head_dim)).astype(jnp.bfloat16)
    group_width = heads * head_dim // N_TP
    attended = jnp.zeros((TOKEN_COUNT, D), jnp.float32)
    for group_index in range(N_TP):
        lo_col = group_index * group_width
        group_term = jnp.dot(mixed[:, lo_col:lo_col + group_width], out_weight[lo_col:lo_col + group_width], preferred_element_type=jnp.float32)
        attended = attended + lax.optimization_barrier(group_term.astype(jnp.bfloat16)).astype(jnp.float32)
    residual = stream.astype(jnp.float32) + attended
    normed = (residual * lax.rsqrt(lax.optimization_barrier(jnp.mean(residual * residual, axis=-1, keepdims=True)) + epsilon) * norm_gain.astype(jnp.float32)).astype(jnp.bfloat16)
    gate_sum = jnp.dot(normed, gate_weight, preferred_element_type=jnp.float32)
    up_sum = jnp.dot(normed, up_weight, preferred_element_type=jnp.float32)
    hidden = (jax.nn.silu(gate_sum) * up_sum).astype(jnp.bfloat16)
    unit_width = FF // N_TP
    mixer_out = jnp.zeros((TOKEN_COUNT, D), jnp.float32)
    for group_index in range(N_TP):
        lo_unit = group_index * unit_width
        group_term = jnp.dot(hidden[:, lo_unit:lo_unit + unit_width], down_weight[lo_unit:lo_unit + unit_width], preferred_element_type=jnp.float32)
        mixer_out = mixer_out + lax.optimization_barrier(group_term.astype(jnp.bfloat16)).astype(jnp.float32)
    return (residual + mixer_out).astype(jnp.bfloat16)
```

```python
import functools

import jax
import jax.numpy as jnp
from jax import lax
from jax.experimental import pallas as pl
from jax.experimental.pallas import tpu as pltpu
from jax.sharding import Mesh
from jax.sharding import PartitionSpec as P

Z, Y = "z", ("y1", "y0")
SP = ("z", "y1", "y0")
TP = ("x", "c")
GROUP = ("y0", "x")
SIZES = {"z": 16, "y1": 2, "y0": 2, "x": 4, "c": 2}
EPS = 1e-6
F32, BF16 = jnp.float32, jnp.bfloat16


def vmem(count):
    return [pl.BlockSpec(memory_space=pltpu.VMEM)] * count


def kernel_cost(flops, moved, exps=0):
    return pl.CostEstimate(flops=flops, bytes_accessed=moved, transcendentals=exps)


def dot(a, b):
    return jnp.dot(a, b, preferred_element_type=F32)


def dot_nt(a, b):
    return lax.dot_general(a, b, (((1,), (1,)), ((), ())), preferred_element_type=F32)


def dot_tn(a, b):
    return lax.dot_general(a, b, (((0,), (0,)), ((), ())), preferred_element_type=F32)


def retention_kernel(q_ref, k_ref, v_ref, decay_ref, within_ref, carry_q_ref, state_ref):
    rows, head_dim = q_ref.shape
    scale = head_dim**-0.5
    at = lax.broadcasted_iota(jnp.int32, (rows, rows), 0)
    to = lax.broadcasted_iota(jnp.int32, (rows, rows), 1)
    causal = at >= to
    running = jnp.sum(jnp.where(causal, decay_ref[...], 0.0), axis=1, keepdims=True)
    across = jnp.sum(jnp.where(at == to, running, 0.0), axis=0, keepdims=True)
    total = running[rows - 1 : rows, :]
    q, k, v = q_ref[...], k_ref[...], v_ref[...]
    table = jnp.where(causal, jnp.exp(jnp.minimum(running - across, 0.0)), 0.0)
    scores = dot_nt(q, k) * scale
    within_ref[...] = dot((scores * table).astype(BF16), v)
    carry_q_ref[...] = (q.astype(F32) * jnp.exp(running)).astype(BF16)
    key_wide = (k.astype(F32) * scale * jnp.exp(total - running)).astype(BF16)
    state = dot_tn(key_wide, v)
    fill = jnp.broadcast_to(total, (8, head_dim))
    slices = state_ref.shape[0]
    part = head_dim // slices
    for n in range(slices):
        state_ref[n, :part, :] = state[n * part : (n + 1) * part]
        state_ref[n, part:, :] = fill


def retention(q, k, v, decay):
    rows, head_dim = q.shape
    part = head_dim // 4
    return pl.pallas_call(
        retention_kernel,
        out_shape=(
            jax.ShapeDtypeStruct((rows, head_dim), F32),
            jax.ShapeDtypeStruct((rows, head_dim), BF16),
            jax.ShapeDtypeStruct((4, part + 8, head_dim), F32),
        ),
        in_specs=vmem(4),
        out_specs=vmem(3),
        cost_estimate=kernel_cost(6 * rows * rows * head_dim, 2**20, rows * rows),
        name="retention",
    )(q, k, v, decay)


def plane_kernel(states_ref, out_ref):
    part = states_ref.shape[1] - 8
    state = states_ref[0, :part, :]
    total = states_ref[0, part : part + 1, :]
    for n in range(1, states_ref.shape[0]):
        own = states_ref[n, part : part + 1, :]
        state = jnp.exp(own) * state + states_ref[n, :part, :]
        total = total + own
    high = total.astype(BF16)
    rest = total - high.astype(F32)
    mid = rest.astype(BF16)
    low = (rest - mid.astype(F32)).astype(BF16)
    line = lax.broadcasted_iota(jnp.int32, (16, total.shape[1]), 0)
    spread = jnp.where(
        line == 0,
        high.astype(F32),
        jnp.where(line == 1, mid.astype(F32), jnp.where(line == 2, low.astype(F32), 0.0)),
    ).astype(BF16)
    packed = state.astype(BF16)
    for n in range(out_ref.shape[0]):
        out_ref[n, :part, :] = packed
        out_ref[n, part:, :] = spread


def plane_state(states):
    count, lines, width = states.shape
    return pl.pallas_call(
        plane_kernel,
        out_shape=jax.ShapeDtypeStruct((16, lines - 8 + 16, width), BF16),
        in_specs=vmem(1),
        out_specs=pl.BlockSpec(memory_space=pltpu.VMEM),
        cost_estimate=kernel_cost(2**18, 2**18, 2**10),
        name="plane_state",
    )(states)


def incoming_kernel(here_ref, planes_ref, states_ref, out_ref):
    part = out_ref.shape[1]
    here = here_ref[0]
    carried = jnp.zeros(out_ref.shape[1:], F32)
    for n in range(planes_ref.shape[0]):
        tail = planes_ref[n, part:, :].astype(F32)
        total = tail[0:1] + tail[1:2] + tail[2:3]
        after = jnp.exp(total) * carried + planes_ref[n, :part, :].astype(F32)
        carried = jnp.where(n < here, after, carried)
    for n in range(out_ref.shape[0]):
        out_ref[n] = carried
        own = states_ref[n, part : part + 1, :]
        carried = jnp.exp(own) * carried + states_ref[n, :part, :]


def incoming_state(here, planes, states):
    count, lines, width = states.shape
    return pl.pallas_call(
        incoming_kernel,
        out_shape=jax.ShapeDtypeStruct((count, lines - 8, width), F32),
        in_specs=[pl.BlockSpec(memory_space=pltpu.SMEM)] + vmem(2),
        out_specs=pl.BlockSpec(memory_space=pltpu.VMEM),
        cost_estimate=kernel_cost(2**19, 2**19, 2**12),
        name="incoming_state",
    )(here, planes, states)


def project_kernel(within_ref, carry_q_ref, state_ref, gate_ref, gain_ref, weight_ref, out_ref):
    retained = within_ref[...] + dot(carry_q_ref[...], state_ref[...].astype(BF16))
    center = jnp.mean(retained, axis=-1, keepdims=True)
    off = retained - center
    spread = jnp.mean(off * off, axis=-1, keepdims=True)
    normed = off * lax.rsqrt(spread + EPS) * gain_ref[...].astype(F32)
    gate = gate_ref[...].astype(F32)
    mixed = (gate * jax.nn.sigmoid(gate) * normed).astype(BF16)
    out_ref[...] = dot(mixed, weight_ref[...]).astype(BF16)


def project(within, carry_q, state, gate, gain, weight):
    rows, width = within.shape[0], weight.shape[1]
    return pl.pallas_call(
        project_kernel,
        out_shape=jax.ShapeDtypeStruct((rows, width), BF16),
        in_specs=vmem(6),
        out_specs=pl.BlockSpec(memory_space=pltpu.VMEM),
        cost_estimate=kernel_cost(2 * rows * 128 * (width + 128), 2**21, rows * 128),
        name="project",
    )(within, carry_q, state, gate, gain, weight)


CHUNKS = 4


def ffn_kernel(rows_ref, weight_ref, out_ref, held, sems):
    z, _, _, kinds, lines, hidden_width = weight_ref.shape
    each = z // CHUNKS
    depth = each * 4 * lines

    def copies(kind, n):
        span = pl.ds(n * each, each)
        return [
            pltpu.make_async_copy(
                weight_ref.at[span, y0, y1, kind],
                held.at[kind, span, y1, y0],
                sems.at[kind, n, 2 * y1 + y0],
            )
            for y1 in range(2)
            for y0 in range(2)
        ]

    for n in range(CHUNKS):
        for kind in (0, 1):
            for copy in copies(kind, n):
                copy.start()
    for n in range(CHUNKS):
        for copy in copies(2, n):
            copy.start()

    def block(kind, n):
        return held[kind, n * each : (n + 1) * each].reshape(depth, hidden_width)

    gate_sum = up_sum = None
    for n in range(CHUNKS):
        for kind in (0, 1):
            for copy in copies(kind, n):
                copy.wait()
        rows = rows_ref[:, n * depth : (n + 1) * depth]
        gate_part, up_part = dot(rows, block(0, n)), dot(rows, block(1, n))
        gate_sum = gate_part if gate_sum is None else gate_sum + gate_part
        up_sum = up_part if up_sum is None else up_sum + up_part
    hidden = (gate_sum * jax.nn.sigmoid(gate_sum) * up_sum).astype(BF16)
    for n in range(CHUNKS):
        for copy in copies(2, n):
            copy.wait()
        out_ref[:, n * depth : (n + 1) * depth] = dot_nt(hidden, block(2, n)).astype(BF16)


def feed_forward(rows, weights):
    count, width = rows.shape
    z, y0, y1, kinds, lines, hidden_width = weights.shape
    return pl.pallas_call(
        ffn_kernel,
        out_shape=jax.ShapeDtypeStruct((count, width), BF16),
        in_specs=[
            pl.BlockSpec(memory_space=pltpu.VMEM),
            pl.BlockSpec(memory_space=pl.ANY),
        ],
        out_specs=pl.BlockSpec(memory_space=pltpu.VMEM),
        scratch_shapes=[
            pltpu.VMEM((kinds, z, y1, y0, lines, hidden_width), BF16),
            pltpu.SemaphoreType.DMA((kinds, CHUNKS, 4)),
        ],
        cost_estimate=kernel_cost(6 * count * width * hidden_width, 2**23, count * hidden_width),
        name="feed_forward",
    )(rows, weights)


def moved(value, axes, place):
    lengths = [SIZES[a] for a in axes]
    pairs = []
    for y1 in range(lengths[0]):
        for y0 in range(lengths[1]):
            for c in range(lengths[2]):
                a, b, d = place(y1, y0, c)
                pairs.append(((y1 * 2 + y0) * 2 + c, (a * 2 + b) * 2 + d))
    return lax.ppermute(value, axes, pairs)


def exchange(tiles, axes):
    return lax.all_to_all(tiles, axes, split_axis=0, concat_axis=0, tiled=True)


def copies_to(value, axes, count):
    return exchange(jnp.broadcast_to(value, (count, *value.shape)), axes)


def gathered_weights(gate_weight, up_weight, down_weight):
    mine = jnp.concatenate([gate_weight, up_weight, down_weight.T], axis=0)
    lines, width = mine.shape
    axes = ("y1", "y0", "c")
    near = moved(mine, axes, lambda y1, y0, c: (y1, c, y0))
    far = moved(mine, axes, lambda y1, y0, c: (1 - y1, c, y0))
    upper = lax.axis_index("y1") == 1
    pair = jnp.stack([jnp.where(upper, far, near), jnp.where(upper, near, far)])
    whole = lax.all_gather(pair, (Z, "c"), axis=0)
    return whole.reshape(16, 2, 2, 3, lines // 3, width)


def local(
    stream,
    queries,
    keys_in,
    values_in,
    gate_in,
    log_decay,
    head_gain,
    out_weight,
    norm_gain,
    gate_weight,
    up_weight,
    down_weight,
):
    weights = gathered_weights(gate_weight, up_weight, down_weight)
    rows = queries.shape[0]
    within, carry_q, state = retention(
        queries, keys_in, values_in, log_decay.reshape(1, rows)
    )
    states = exchange(state, Y)
    planes = exchange(plane_state(states), Z)
    here = lax.axis_index(Z).astype(jnp.int32).reshape(1)
    entering = exchange(incoming_state(here, planes, states), Y)
    entering = entering.reshape(queries.shape[1], queries.shape[1])
    terms = project(within, carry_q, entering, gate_in, head_gain.reshape(1, -1), out_weight)
    width = terms.shape[1]
    attended = exchange(terms.reshape(8, rows // 8, width), TP).astype(F32).sum(axis=0)
    residual = stream.astype(F32) + attended
    normed = (
        residual
        * lax.rsqrt(jnp.mean(residual * residual, axis=-1, keepdims=True) + EPS)
        * norm_gain.astype(F32)
    ).astype(BF16)
    group_rows = copies_to(normed, GROUP, 8).reshape(rows, width)
    down_terms = feed_forward(group_rows, weights)
    mixer_out = exchange(down_terms.reshape(8, rows // 8, width), GROUP).astype(F32).sum(axis=0)
    return (residual + mixer_out).astype(BF16)


def solution(mesh):
    finer = Mesh(mesh.devices.reshape(*SIZES.values()), tuple(SIZES))
    return jax.shard_map(
        local,
        mesh=finer,
        in_specs=(
            P(SP + TP, None),
            P(SP, TP),
            P(SP, TP),
            P(SP, TP),
            P(SP, TP),
            P(SP, TP),
            P(TP),
            P(TP, None),
            P(),
            P(SP, TP),
            P(SP, TP),
            P(TP, SP),
        ),
        out_specs=P(SP + TP, None),
        check_vma=False,
    )
```

```python
import jax
import jax.numpy as jnp
from jax import lax
from jax.experimental import pallas as pl
from jax.experimental.pallas import tpu as pltpu
from jax.sharding import Mesh
from jax.sharding import PartitionSpec as P


Z, Y = "z", ("y1", "y0")
SP = ("z", "y1", "y0")
TP = ("x", "c")
GROUP = ("y0", "x")
SIZES = {"z": 16, "y1": 2, "y0": 2, "x": 4, "c": 2}
EPS = 1e-6
F32, BF16 = jnp.float32, jnp.bfloat16


def vmem(count):
    return [pl.BlockSpec(memory_space=pltpu.VMEM)] * count


def kernel_cost(flops, moved, exps=0):
    return pl.CostEstimate(flops=flops, bytes_accessed=moved, transcendentals=exps)


def dot(a, b):
    return jnp.dot(a, b, preferred_element_type=F32)


def dot_nt(a, b):
    return lax.dot_general(a, b, (((1,), (1,)), ((), ())), preferred_element_type=F32)


def dot_tn(a, b):
    return lax.dot_general(a, b, (((0,), (0,)), ((), ())), preferred_element_type=F32)


def retention_kernel(q_ref, k_ref, v_ref, decay_ref, within_ref, carry_q_ref, state_ref):
    rows, head_dim = q_ref.shape
    scale = head_dim**-0.5
    at = lax.broadcasted_iota(jnp.int32, (rows, rows), 0)
    to = lax.broadcasted_iota(jnp.int32, (rows, rows), 1)
    causal = at >= to
    running = jnp.sum(jnp.where(causal, decay_ref[...], 0.0), axis=1, keepdims=True)
    across = jnp.sum(jnp.where(at == to, running, 0.0), axis=0, keepdims=True)
    total = running[rows - 1 : rows, :]
    q, k, v = q_ref[...], k_ref[...], v_ref[...]
    table = jnp.where(causal, jnp.exp(jnp.minimum(running - across, 0.0)), 0.0)
    scores = dot_nt(q, k) * scale
    within_ref[...] = dot((scores * table).astype(BF16), v)
    carry_q_ref[...] = (q.astype(F32) * jnp.exp(running)).astype(BF16)
    key_wide = (k.astype(F32) * scale * jnp.exp(total - running)).astype(BF16)
    state = dot_tn(key_wide, v)
    fill = jnp.broadcast_to(total, (8, head_dim))
    slices = state_ref.shape[0]
    part = head_dim // slices
    for n in range(slices):
        state_ref[n, :part, :] = state[n * part : (n + 1) * part]
        state_ref[n, part:, :] = fill


def retention(q, k, v, decay):
    rows, head_dim = q.shape
    part = head_dim // 4
    return pl.pallas_call(
        retention_kernel,
        out_shape=(
            jax.ShapeDtypeStruct((rows, head_dim), F32),
            jax.ShapeDtypeStruct((rows, head_dim), BF16),
            jax.ShapeDtypeStruct((4, part + 8, head_dim), F32),
        ),
        in_specs=vmem(4),
        out_specs=vmem(3),
        cost_estimate=kernel_cost(6 * rows * rows * head_dim, 2**20, rows * rows),
        name="retention",
    )(q, k, v, decay)


def plane_kernel(states_ref, out_ref):
    part = states_ref.shape[1] - 8
    state = states_ref[0, :part, :]
    total = states_ref[0, part : part + 1, :]
    for n in range(1, states_ref.shape[0]):
        own = states_ref[n, part : part + 1, :]
        state = jnp.exp(own) * state + states_ref[n, :part, :]
        total = total + own
    high = total.astype(BF16)
    rest = total - high.astype(F32)
    mid = rest.astype(BF16)
    low = (rest - mid.astype(F32)).astype(BF16)
    line = lax.broadcasted_iota(jnp.int32, (16, total.shape[1]), 0)
    spread = jnp.where(
        line == 0,
        high.astype(F32),
        jnp.where(line == 1, mid.astype(F32), jnp.where(line == 2, low.astype(F32), 0.0)),
    ).astype(BF16)
    packed = state.astype(BF16)
    for n in range(out_ref.shape[0]):
        out_ref[n, :part, :] = packed
        out_ref[n, part:, :] = spread


def plane_state(states):
    _, lines, width = states.shape
    return pl.pallas_call(
        plane_kernel,
        out_shape=jax.ShapeDtypeStruct((16, lines - 8 + 16, width), BF16),
        in_specs=vmem(1),
        out_specs=pl.BlockSpec(memory_space=pltpu.VMEM),
        cost_estimate=kernel_cost(2**18, 2**18, 2**10),
        name="plane_state",
    )(states)


def incoming_kernel(here_ref, planes_ref, states_ref, out_ref):
    part = out_ref.shape[1]
    here = here_ref[0]
    carried = jnp.zeros(out_ref.shape[1:], F32)
    for n in range(planes_ref.shape[0]):
        tail = planes_ref[n, part:, :].astype(F32)
        total = tail[0:1] + tail[1:2] + tail[2:3]
        after = jnp.exp(total) * carried + planes_ref[n, :part, :].astype(F32)
        carried = jnp.where(n < here, after, carried)
    for n in range(out_ref.shape[0]):
        out_ref[n] = carried
        own = states_ref[n, part : part + 1, :]
        carried = jnp.exp(own) * carried + states_ref[n, :part, :]


def incoming_state(here, planes, states):
    count, lines, width = states.shape
    return pl.pallas_call(
        incoming_kernel,
        out_shape=jax.ShapeDtypeStruct((count, lines - 8, width), F32),
        in_specs=[pl.BlockSpec(memory_space=pltpu.SMEM)] + vmem(2),
        out_specs=pl.BlockSpec(memory_space=pltpu.VMEM),
        cost_estimate=kernel_cost(2**19, 2**19, 2**12),
        name="incoming_state",
    )(here, planes, states)


def mix_kernel(within_ref, carry_q_ref, state_ref, gate_ref, gain_ref, out_ref):
    retained = within_ref[...] + dot(carry_q_ref[...], state_ref[...].astype(BF16))
    center = jnp.mean(retained, axis=-1, keepdims=True)
    off = retained - center
    spread = jnp.mean(off * off, axis=-1, keepdims=True)
    normed = off * lax.rsqrt(spread + EPS) * gain_ref[...].astype(F32)
    gate = gate_ref[...].astype(F32)
    mixed = (gate * jax.nn.sigmoid(gate) * normed).astype(BF16)
    places, cores, blocks, lines, _ = out_ref.shape
    for core in range(cores):
        for n in range(blocks):
            first = (n * cores + core) * lines
            piece = mixed[first : first + lines]
            for place in range(places):
                out_ref[place, core, n] = piece


def mix(within, carry_q, state, gate, gain):
    rows, width = within.shape
    return pl.pallas_call(
        mix_kernel,
        out_shape=jax.ShapeDtypeStruct((8, 2, 4, rows // 8, width), BF16),
        in_specs=vmem(5),
        out_specs=pl.BlockSpec(memory_space=pltpu.VMEM),
        cost_estimate=kernel_cost(2 * rows * width * width, 2**20, rows * width),
        name="mix",
    )(within, carry_q, state, gate, gain)


def rows_kernel(
    here_ref, mixed_ref, near_w_ref, far_w_ref, near_s_ref, far_s_ref, gain_ref, normed_ref, own_ref, residual
):
    halves, _, blocks, lines, head_dim = mixed_ref.shape
    count, width = normed_ref.shape
    x, c, y0 = here_ref[0], here_ref[1], here_ref[2]

    def heads_of(core):
        return jnp.concatenate(
            [
                jnp.concatenate(
                    [mixed_ref[n, ((x + 4 - r) % 4) * 2 + core].reshape(count // halves, head_dim) for r in range(4)],
                    axis=1,
                )
                for n in range(halves)
            ],
            axis=0,
        )

    near, far = heads_of(c), heads_of(1 - c)
    step = width // 4
    squares = jnp.zeros((count, 1), F32)
    for n in range(4):
        span = slice(n * step, (n + 1) * step)
        rows = []
        for half in range(halves):
            for block in range(blocks):
                at = (x + 4 - block) % 4
                rows.append(jnp.where(y0 == half, near_s_ref[at, :, span], far_s_ref[at, :, span]))
        part = (
            jnp.concatenate(rows, axis=0).astype(F32)
            + dot(near, near_w_ref[:, span])
            + dot(far, far_w_ref[:, span])
        )
        residual[:, span] = part
        squares += jnp.sum(part * part, axis=-1, keepdims=True)
    factor = lax.rsqrt(squares / width + EPS)
    for n in range(4):
        span = slice(n * step, (n + 1) * step)
        normed_ref[:, span] = (residual[:, span] * factor * gain_ref[:, span].astype(F32)).astype(BF16)
    first = pl.multiple_of((y0 * blocks + x) * lines, lines)
    own_ref[...] = residual[pl.ds(first, lines), :]


def group_rows(here, mixed, near_w, far_w, near_s, far_s, gain):
    lines, width = near_s.shape[1:]
    count = 8 * lines
    return pl.pallas_call(
        rows_kernel,
        out_shape=(
            jax.ShapeDtypeStruct((count, width), BF16),
            jax.ShapeDtypeStruct((lines, width), F32),
        ),
        in_specs=[pl.BlockSpec(memory_space=pltpu.SMEM)] + vmem(6),
        out_specs=vmem(2),
        scratch_shapes=[pltpu.VMEM((count, width), F32)],
        cost_estimate=kernel_cost(2 * count * width * 1024, 2**23),
        name="group_rows",
    )(here, mixed, near_w, far_w, near_s, far_s, gain)


CHUNKS = 4


def ffn_kernel(rows_ref, weight_ref, out_ref, held, sems):
    z, _, _, _, lines, hidden_width = weight_ref.shape
    each = z // CHUNKS
    depth = each * 4 * lines

    def copies(kind, n):
        span = pl.ds(n * each, each)
        return [
            pltpu.make_async_copy(
                weight_ref.at[span, y0, y1, kind],
                held.at[kind, span, y1, y0],
                sems.at[kind, n, 2 * y1 + y0],
            )
            for y1 in range(2)
            for y0 in range(2)
        ]

    for n in range(CHUNKS):
        for kind in (0, 1):
            for copy in copies(kind, n):
                copy.start()
    for n in range(CHUNKS):
        for copy in copies(2, n):
            copy.start()

    def block(kind, n):
        return held[kind, n * each : (n + 1) * each].reshape(depth, hidden_width)

    gate_sum = up_sum = None
    for n in range(CHUNKS):
        for kind in (0, 1):
            for copy in copies(kind, n):
                copy.wait()
        rows = rows_ref[:, n * depth : (n + 1) * depth]
        gate_part, up_part = dot(rows, block(0, n)), dot(rows, block(1, n))
        gate_sum = gate_part if gate_sum is None else gate_sum + gate_part
        up_sum = up_part if up_sum is None else up_sum + up_part
    hidden = (gate_sum * jax.nn.sigmoid(gate_sum) * up_sum).astype(BF16)
    for n in range(CHUNKS):
        for copy in copies(2, n):
            copy.wait()
        out_ref[:, n * depth : (n + 1) * depth] = dot_nt(hidden, block(2, n)).astype(BF16)


def feed_forward(rows, weights):
    count, width = rows.shape
    z, y0, y1, kinds, lines, hidden_width = weights.shape
    return pl.pallas_call(
        ffn_kernel,
        out_shape=jax.ShapeDtypeStruct((count, width), BF16),
        in_specs=[
            pl.BlockSpec(memory_space=pltpu.VMEM),
            pl.BlockSpec(memory_space=pl.ANY),
        ],
        out_specs=pl.BlockSpec(memory_space=pltpu.VMEM),
        scratch_shapes=[
            pltpu.VMEM((kinds, z, y1, y0, lines, hidden_width), BF16),
            pltpu.SemaphoreType.DMA((kinds, CHUNKS, 4)),
        ],
        cost_estimate=kernel_cost(6 * count * width * hidden_width, 2**23, count * hidden_width),
        name="feed_forward",
    )(rows, weights)


def moved(value, axes, place):
    lengths = [SIZES[a] for a in axes]
    pairs = []
    for y1 in range(lengths[0]):
        for y0 in range(lengths[1]):
            for c in range(lengths[2]):
                a, b, d = place(y1, y0, c)
                pairs.append(((y1 * 2 + y0) * 2 + c, (a * 2 + b) * 2 + d))
    return lax.ppermute(value, axes, pairs)


def shifted(value, axis, by):
    length = SIZES[axis]
    return lax.ppermute(value, axis, [(i, (i + by) % length) for i in range(length)])


def exchange(tiles, axes):
    return lax.all_to_all(tiles, axes, split_axis=0, concat_axis=0, tiled=True)


def gathered_weights(gate_weight, up_weight, down_weight):
    mine = jnp.concatenate([gate_weight, up_weight, down_weight.T], axis=0)
    lines, width = mine.shape
    axes = ("y1", "y0", "c")
    near = moved(mine, axes, lambda y1, y0, c: (y1, c, y0))
    far = moved(mine, axes, lambda y1, y0, c: (1 - y1, c, y0))
    upper = lax.axis_index("y1") == 1
    pair = jnp.stack([jnp.where(upper, far, near), jnp.where(upper, near, far)])
    whole = lax.all_gather(pair, (Z, "c"), axis=0)
    return whole.reshape(16, 2, 2, 3, lines // 3, width), pair


def layer(
    stream,
    queries,
    keys_in,
    values_in,
    gate_in,
    log_decay,
    head_gain,
    out_weight,
    norm_gain,
    gate_weight,
    up_weight,
    down_weight,
):
    weights, tied = gathered_weights(gate_weight, up_weight, down_weight)
    rows, width = queries.shape[0], stream.shape[1]
    head_dim = queries.shape[1]
    block = jnp.concatenate([out_weight, stream], axis=0)
    block, _ = lax.optimization_barrier((block, tied))
    found = [block] + [shifted(block, "x", r) for r in (1, 2, 3)]
    near_w = jnp.concatenate([b[:head_dim] for b in found], axis=0)
    near_s = jnp.stack([b[head_dim:] for b in found])
    far_w = shifted(near_w, "c", 1)
    far_s = shifted(near_s, "y0", 1)
    within, carry_q, state = retention(
        queries, keys_in, values_in, log_decay.reshape(1, rows)
    )
    states = exchange(state, Y)
    packed = plane_state(states)
    planes = exchange(packed, Z)
    here = lax.axis_index(Z).astype(jnp.int32).reshape(1)
    entering = incoming_state(here, planes, states)
    entering = exchange(entering, Y)
    entering = entering.reshape(queries.shape[1], queries.shape[1])
    sent = mix(within, carry_q, entering, gate_in, head_gain.reshape(1, -1))
    mixed = exchange(sent.reshape(16, *sent.shape[2:]), GROUP + ("c",))
    here = jnp.stack([lax.axis_index(a).astype(jnp.int32) for a in ("x", "c", "y0")])
    normed, residual = group_rows(
        here, mixed.reshape(2, 8, *mixed.shape[1:]), near_w, far_w, near_s, far_s, norm_gain.reshape(1, -1)
    )
    down_terms = feed_forward(normed, weights)
    mixer_out = exchange(down_terms.reshape(8, rows // 8, width), GROUP).astype(F32).sum(axis=0)
    return (residual + mixer_out).astype(BF16)


def solution(mesh):
    finer = Mesh(mesh.devices.reshape(*SIZES.values()), tuple(SIZES))
    return jax.shard_map(
        layer,
        mesh=finer,
        in_specs=(
            P(SP + TP, None),
            P(SP, TP),
            P(SP, TP),
            P(SP, TP),
            P(SP, TP),
            P(SP, TP),
            P(TP),
            P(TP, None),
            P(),
            P(SP, TP),
            P(SP, TP),
            P(TP, SP),
        ),
        out_specs=P(SP + TP, None),
        check_vma=False,
    )
```

```python
import jax
import jax.numpy as jnp
from jax import lax
from jax.experimental import pallas as pl
from jax.experimental.pallas import tpu as pltpu
from jax.sharding import Mesh
from jax.sharding import PartitionSpec as P


Z, Y = ("zh", "zl"), ("y1", "y0")
NEAR = ("zl",) + Y
SP = Z + Y
TP = ("x", "c")
GROUP = ("y0", "x")
SIZES = {"zh": 4, "zl": 4, "y1": 2, "y0": 2, "x": 4, "c": 2}
EPS = 1e-6
F32, BF16 = jnp.float32, jnp.bfloat16


def vmem(count):
    return [pl.BlockSpec(memory_space=pltpu.VMEM)] * count


def kernel_cost(flops, moved, exps=0):
    return pl.CostEstimate(flops=flops, bytes_accessed=moved, transcendentals=exps)


def dot(a, b):
    return jnp.dot(a, b, preferred_element_type=F32)


def dot_nt(a, b):
    return lax.dot_general(a, b, (((1,), (1,)), ((), ())), preferred_element_type=F32)


def dot_tn(a, b):
    return lax.dot_general(a, b, (((0,), (0,)), ((), ())), preferred_element_type=F32)


def retention_kernel(q_ref, k_ref, v_ref, decay_ref, within_ref, carry_q_ref, state_ref):
    rows, head_dim = q_ref.shape
    scale = head_dim**-0.5
    at = lax.broadcasted_iota(jnp.int32, (rows, rows), 0)
    to = lax.broadcasted_iota(jnp.int32, (rows, rows), 1)
    causal = at >= to
    running = jnp.sum(jnp.where(causal, decay_ref[...], 0.0), axis=1, keepdims=True)
    across = jnp.sum(jnp.where(at == to, running, 0.0), axis=0, keepdims=True)
    total = running[rows - 1 : rows, :]
    q, k, v = q_ref[...], k_ref[...], v_ref[...]
    table = jnp.where(causal, jnp.exp(jnp.minimum(running - across, 0.0)), 0.0)
    scores = dot_nt(q, k) * scale
    within_ref[...] = dot((scores * table).astype(BF16), v)
    carry_q_ref[...] = (q.astype(F32) * jnp.exp(running)).astype(BF16)
    key_wide = (k.astype(F32) * scale * jnp.exp(total - running)).astype(BF16)
    state = dot_tn(key_wide, v)
    fill = jnp.broadcast_to(total, (8, head_dim))
    slices = state_ref.shape[0]
    part = head_dim // slices
    for n in range(slices):
        state_ref[n, :part, :] = state[n * part : (n + 1) * part]
        state_ref[n, part:, :] = fill


def retention(q, k, v, decay):
    rows, head_dim = q.shape
    part = head_dim // 16
    return pl.pallas_call(
        retention_kernel,
        out_shape=(
            jax.ShapeDtypeStruct((rows, head_dim), F32),
            jax.ShapeDtypeStruct((rows, head_dim), BF16),
            jax.ShapeDtypeStruct((16, part + 8, head_dim), F32),
        ),
        in_specs=vmem(4),
        out_specs=vmem(3),
        cost_estimate=kernel_cost(6 * rows * rows * head_dim, 2**20, rows * rows),
        name="retention",
    )(q, k, v, decay)


def joined_kernel(states_ref, out_ref):
    part = states_ref.shape[1] - 8
    state = states_ref[0, :part, :]
    total = states_ref[0, part:, :]
    for n in range(1, states_ref.shape[0]):
        own = states_ref[n, part:, :]
        state = jnp.exp(own) * state + states_ref[n, :part, :]
        total = total + own
    for n in range(out_ref.shape[0]):
        out_ref[n, :part, :] = state
        out_ref[n, part:, :] = total


def joined_state(states):
    _, lines, width = states.shape
    return pl.pallas_call(
        joined_kernel,
        out_shape=jax.ShapeDtypeStruct((4, lines, width), F32),
        in_specs=vmem(1),
        out_specs=pl.BlockSpec(memory_space=pltpu.VMEM),
        cost_estimate=kernel_cost(2**18, 2**18, 2**10),
        name="joined_state",
    )(states)


def incoming_kernel(here_ref, joined_ref, states_ref, out_ref):
    part = out_ref.shape[1]
    here = here_ref[0]
    carried = jnp.zeros(out_ref.shape[1:], F32)
    for n in range(joined_ref.shape[0]):
        after = jnp.exp(joined_ref[n, part:, :]) * carried + joined_ref[n, :part, :]
        carried = jnp.where(n < here, after, carried)
    for n in range(out_ref.shape[0]):
        out_ref[n] = carried
        carried = jnp.exp(states_ref[n, part:, :]) * carried + states_ref[n, :part, :]


def incoming_state(here, joined, states):
    count, lines, width = states.shape
    return pl.pallas_call(
        incoming_kernel,
        out_shape=jax.ShapeDtypeStruct((count, lines - 8, width), F32),
        in_specs=[pl.BlockSpec(memory_space=pltpu.SMEM)] + vmem(2),
        out_specs=pl.BlockSpec(memory_space=pltpu.VMEM),
        cost_estimate=kernel_cost(2**19, 2**19, 2**12),
        name="incoming_state",
    )(here, joined, states)


def mix_kernel(within_ref, carry_q_ref, state_ref, gate_ref, gain_ref, out_ref):
    retained = within_ref[...] + dot(carry_q_ref[...], state_ref[...].astype(BF16))
    center = jnp.mean(retained, axis=-1, keepdims=True)
    off = retained - center
    spread = jnp.mean(off * off, axis=-1, keepdims=True)
    normed = off * lax.rsqrt(spread + EPS) * gain_ref[...].astype(F32)
    gate = gate_ref[...].astype(F32)
    mixed = (gate * jax.nn.sigmoid(gate) * normed).astype(BF16)
    places, cores, blocks, lines, _ = out_ref.shape
    for core in range(cores):
        for n in range(blocks):
            first = (n * cores + core) * lines
            piece = mixed[first : first + lines]
            for place in range(places):
                out_ref[place, core, n] = piece


def mix(within, carry_q, state, gate, gain):
    rows, width = within.shape
    return pl.pallas_call(
        mix_kernel,
        out_shape=jax.ShapeDtypeStruct((8, 2, 4, rows // 8, width), BF16),
        in_specs=vmem(5),
        out_specs=pl.BlockSpec(memory_space=pltpu.VMEM),
        cost_estimate=kernel_cost(2 * rows * width * width, 2**20, rows * width),
        name="mix",
    )(within, carry_q, state, gate, gain)


def rows_kernel(
    here_ref, mixed_ref, near_w_ref, far_w_ref, near_s_ref, far_s_ref, gain_ref, normed_ref, own_ref, residual
):
    halves, _, blocks, lines, head_dim = mixed_ref.shape
    count, width = normed_ref.shape
    x, c, y0 = here_ref[0], here_ref[1], here_ref[2]

    def heads_of(core):
        return jnp.concatenate(
            [
                jnp.concatenate(
                    [mixed_ref[n, ((x + 4 - r) % 4) * 2 + core].reshape(count // halves, head_dim) for r in range(4)],
                    axis=1,
                )
                for n in range(halves)
            ],
            axis=0,
        )

    near, far = heads_of(c), heads_of(1 - c)
    step = width // 4
    squares = jnp.zeros((count, 1), F32)
    for n in range(4):
        span = slice(n * step, (n + 1) * step)
        rows = []
        for half in range(halves):
            for block in range(blocks):
                at = (x + 4 - block) % 4
                rows.append(jnp.where(y0 == half, near_s_ref[at, :, span], far_s_ref[at, :, span]))
        part = (
            jnp.concatenate(rows, axis=0).astype(F32)
            + dot(near, near_w_ref[:, span])
            + dot(far, far_w_ref[:, span])
        )
        residual[:, span] = part
        squares += jnp.sum(part * part, axis=-1, keepdims=True)
    factor = lax.rsqrt(squares / width + EPS)
    for n in range(4):
        span = slice(n * step, (n + 1) * step)
        normed_ref[:, span] = (residual[:, span] * factor * gain_ref[:, span].astype(F32)).astype(BF16)
    first = pl.multiple_of((y0 * blocks + x) * lines, lines)
    own_ref[...] = residual[pl.ds(first, lines), :]


def group_rows(here, mixed, near_w, far_w, near_s, far_s, gain):
    lines, width = near_s.shape[1:]
    count = 8 * lines
    return pl.pallas_call(
        rows_kernel,
        out_shape=(
            jax.ShapeDtypeStruct((count, width), BF16),
            jax.ShapeDtypeStruct((lines, width), F32),
        ),
        in_specs=[pl.BlockSpec(memory_space=pltpu.SMEM)] + vmem(6),
        out_specs=vmem(2),
        scratch_shapes=[pltpu.VMEM((count, width), F32)],
        cost_estimate=kernel_cost(2 * count * width * 1024, 2**23),
        name="group_rows",
    )(here, mixed, near_w, far_w, near_s, far_s, gain)


CHUNKS = 4


def ffn_kernel(rows_ref, weight_ref, out_ref, held, sems):
    z, _, _, _, lines, hidden_width = weight_ref.shape
    each = z // CHUNKS
    depth = each * 4 * lines

    def copies(kind, n):
        span = pl.ds(n * each, each)
        return [
            pltpu.make_async_copy(
                weight_ref.at[span, y0, y1, kind],
                held.at[kind, span, y1, y0],
                sems.at[kind, n, 2 * y1 + y0],
            )
            for y1 in range(2)
            for y0 in range(2)
        ]

    for n in range(CHUNKS):
        for kind in (0, 1):
            for copy in copies(kind, n):
                copy.start()
    for n in range(CHUNKS):
        for copy in copies(2, n):
            copy.start()

    def block(kind, n):
        return held[kind, n * each : (n + 1) * each].reshape(depth, hidden_width)

    gate_sum = up_sum = None
    for n in range(CHUNKS):
        for kind in (0, 1):
            for copy in copies(kind, n):
                copy.wait()
        rows = rows_ref[:, n * depth : (n + 1) * depth]
        gate_part, up_part = dot(rows, block(0, n)), dot(rows, block(1, n))
        gate_sum = gate_part if gate_sum is None else gate_sum + gate_part
        up_sum = up_part if up_sum is None else up_sum + up_part
    hidden = (gate_sum * jax.nn.sigmoid(gate_sum) * up_sum).astype(BF16)
    for n in range(CHUNKS):
        for copy in copies(2, n):
            copy.wait()
        out_ref[:, n * depth : (n + 1) * depth] = dot_nt(hidden, block(2, n)).astype(BF16)


def feed_forward(rows, weights):
    count, width = rows.shape
    z, y0, y1, kinds, lines, hidden_width = weights.shape
    return pl.pallas_call(
        ffn_kernel,
        out_shape=jax.ShapeDtypeStruct((count, width), BF16),
        in_specs=[
            pl.BlockSpec(memory_space=pltpu.VMEM),
            pl.BlockSpec(memory_space=pl.ANY),
        ],
        out_specs=pl.BlockSpec(memory_space=pltpu.VMEM),
        scratch_shapes=[
            pltpu.VMEM((kinds, z, y1, y0, lines, hidden_width), BF16),
            pltpu.SemaphoreType.DMA((kinds, CHUNKS, 4)),
        ],
        cost_estimate=kernel_cost(6 * count * width * hidden_width, 2**23, count * hidden_width),
        name="feed_forward",
    )(rows, weights)


def moved(value, axes, place):
    lengths = [SIZES[a] for a in axes]
    pairs = []
    for y1 in range(lengths[0]):
        for y0 in range(lengths[1]):
            for c in range(lengths[2]):
                a, b, d = place(y1, y0, c)
                pairs.append(((y1 * 2 + y0) * 2 + c, (a * 2 + b) * 2 + d))
    return lax.ppermute(value, axes, pairs)


def shifted(value, axis, by):
    length = SIZES[axis]
    return lax.ppermute(value, axis, [(i, (i + by) % length) for i in range(length)])


def exchange(tiles, axes):
    return lax.all_to_all(tiles, axes, split_axis=0, concat_axis=0, tiled=True)


def gathered_weights(gate_weight, up_weight, down_weight):
    mine = jnp.concatenate([gate_weight, up_weight, down_weight.T], axis=0)
    lines, width = mine.shape
    axes = ("y1", "y0", "c")
    near = moved(mine, axes, lambda y1, y0, c: (y1, c, y0))
    far = moved(mine, axes, lambda y1, y0, c: (1 - y1, c, y0))
    upper = lax.axis_index("y1") == 1
    pair = jnp.stack([jnp.where(upper, far, near), jnp.where(upper, near, far)])
    whole = lax.all_gather(pair, Z + ("c",), axis=0)
    return whole.reshape(16, 2, 2, 3, lines // 3, width), pair


def layer(
    stream,
    queries,
    keys_in,
    values_in,
    gate_in,
    log_decay,
    head_gain,
    out_weight,
    norm_gain,
    gate_weight,
    up_weight,
    down_weight,
):
    weights, tied = gathered_weights(gate_weight, up_weight, down_weight)
    rows, width = queries.shape[0], stream.shape[1]
    head_dim = queries.shape[1]
    block = jnp.concatenate([out_weight, stream], axis=0)
    block, _ = lax.optimization_barrier((block, tied))
    found = [block] + [shifted(block, "x", r) for r in (1, 2, 3)]
    near_w = jnp.concatenate([b[:head_dim] for b in found], axis=0)
    near_s = jnp.stack([b[head_dim:] for b in found])
    far_w = shifted(near_w, "c", 1)
    far_s = shifted(near_s, "y0", 1)
    within, carry_q, state = retention(
        queries, keys_in, values_in, log_decay.reshape(1, rows)
    )
    states = exchange(state, NEAR)
    joined = joined_state(states)
    joined = exchange(joined, "zh")
    zh = lax.axis_index("zh").astype(jnp.int32).reshape(1)
    entering = incoming_state(zh, joined, states)
    entering = exchange(entering, NEAR)
    entering = entering.reshape(head_dim, head_dim)
    sent = mix(within, carry_q, entering, gate_in, head_gain.reshape(1, -1))
    mixed = exchange(sent.reshape(16, *sent.shape[2:]), GROUP + ("c",))
    here = jnp.stack([lax.axis_index(a).astype(jnp.int32) for a in ("x", "c", "y0")])
    normed, residual = group_rows(
        here, mixed.reshape(2, 8, *mixed.shape[1:]), near_w, far_w, near_s, far_s, norm_gain.reshape(1, -1)
    )
    down_terms = feed_forward(normed, weights)
    mixer_out = exchange(down_terms.reshape(8, rows // 8, width), GROUP).astype(F32).sum(axis=0)
    return (residual + mixer_out).astype(BF16)


def solution(mesh):
    finer = Mesh(mesh.devices.reshape(*SIZES.values()), tuple(SIZES))
    return jax.shard_map(
        layer,
        mesh=finer,
        in_specs=(
            P(SP + TP, None),
            P(SP, TP),
            P(SP, TP),
            P(SP, TP),
            P(SP, TP),
            P(SP, TP),
            P(TP),
            P(TP, None),
            P(),
            P(SP, TP),
            P(SP, TP),
            P(TP, SP),
        ),
        out_specs=P(SP + TP, None),
        check_vma=False,
    )
```

```python
import jax
import jax.numpy as jnp
from jax import lax
from jax.experimental import pallas as pl
from jax.experimental.pallas import tpu as pltpu
from jax.sharding import Mesh
from jax.sharding import PartitionSpec as P


Z, Y = ("zh", "zl"), ("y1", "y0")
NEAR = ("zl",) + Y
SP = Z + Y
TP = ("x", "c")
GROUP = ("y0", "x")
SIZES = {"zh": 4, "zl": 4, "y1": 2, "y0": 2, "x": 4, "c": 2}
EPS = 1e-6
F32, BF16 = jnp.float32, jnp.bfloat16


def vmem(count):
    return [pl.BlockSpec(memory_space=pltpu.VMEM)] * count


def kernel_cost(flops, moved, exps=0):
    return pl.CostEstimate(flops=flops, bytes_accessed=moved, transcendentals=exps)


def dot(a, b):
    return jnp.dot(a, b, preferred_element_type=F32)


def dot_nt(a, b):
    return lax.dot_general(a, b, (((1,), (1,)), ((), ())), preferred_element_type=F32)


def dot_tn(a, b):
    return lax.dot_general(a, b, (((0,), (0,)), ((), ())), preferred_element_type=F32)


def retention_kernel(q_ref, k_ref, v_ref, decay_ref, within_ref, carry_q_ref, state_ref):
    rows, head_dim = q_ref.shape
    scale = head_dim**-0.5
    at = lax.broadcasted_iota(jnp.int32, (rows, rows), 0)
    to = lax.broadcasted_iota(jnp.int32, (rows, rows), 1)
    causal = at >= to
    running = jnp.sum(jnp.where(causal, decay_ref[...], 0.0), axis=1, keepdims=True)
    across = jnp.sum(jnp.where(at == to, running, 0.0), axis=0, keepdims=True)
    total = running[rows - 1 : rows, :]
    q, k, v = q_ref[...], k_ref[...], v_ref[...]
    table = jnp.where(causal, jnp.exp(jnp.minimum(running - across, 0.0)), 0.0)
    scores = dot_nt(q, k) * scale
    within_ref[...] = dot((scores * table).astype(BF16), v)
    carry_q_ref[...] = (q.astype(F32) * jnp.exp(running)).astype(BF16)
    key_wide = (k.astype(F32) * scale * jnp.exp(total - running)).astype(BF16)
    state = dot_tn(key_wide, v)
    fill = jnp.broadcast_to(total, (8, head_dim))
    slices = state_ref.shape[0]
    part = head_dim // slices
    for n in range(slices):
        state_ref[n, :part, :] = state[n * part : (n + 1) * part]
        state_ref[n, part:, :] = fill


def retention(q, k, v, decay):
    rows, head_dim = q.shape
    part = head_dim // 16
    return pl.pallas_call(
        retention_kernel,
        out_shape=(
            jax.ShapeDtypeStruct((rows, head_dim), F32),
            jax.ShapeDtypeStruct((rows, head_dim), BF16),
            jax.ShapeDtypeStruct((16, part + 8, head_dim), F32),
        ),
        in_specs=vmem(4),
        out_specs=vmem(3),
        cost_estimate=kernel_cost(6 * rows * rows * head_dim, 2**20, rows * rows),
        name="retention",
    )(q, k, v, decay)


def joined_kernel(states_ref, out_ref):
    part = states_ref.shape[1] - 8
    state = states_ref[0, :part, :]
    total = states_ref[0, part:, :]
    for n in range(1, states_ref.shape[0]):
        own = states_ref[n, part:, :]
        state = jnp.exp(own) * state + states_ref[n, :part, :]
        total = total + own
    for n in range(out_ref.shape[0]):
        out_ref[n, :part, :] = state
        out_ref[n, part:, :] = total


def joined_state(states):
    _, lines, width = states.shape
    return pl.pallas_call(
        joined_kernel,
        out_shape=jax.ShapeDtypeStruct((4, lines, width), F32),
        in_specs=vmem(1),
        out_specs=pl.BlockSpec(memory_space=pltpu.VMEM),
        cost_estimate=kernel_cost(2**18, 2**18, 2**10),
        name="joined_state",
    )(states)


def incoming_kernel(here_ref, joined_ref, states_ref, out_ref):
    part = out_ref.shape[1]
    here = here_ref[0]
    carried = jnp.zeros(out_ref.shape[1:], F32)
    for n in range(joined_ref.shape[0]):
        after = jnp.exp(joined_ref[n, part:, :]) * carried + joined_ref[n, :part, :]
        carried = jnp.where(n < here, after, carried)
    for n in range(out_ref.shape[0]):
        out_ref[n] = carried
        carried = jnp.exp(states_ref[n, part:, :]) * carried + states_ref[n, :part, :]


def incoming_state(here, joined, states):
    count, lines, width = states.shape
    return pl.pallas_call(
        incoming_kernel,
        out_shape=jax.ShapeDtypeStruct((count, lines - 8, width), F32),
        in_specs=[pl.BlockSpec(memory_space=pltpu.SMEM)] + vmem(2),
        out_specs=pl.BlockSpec(memory_space=pltpu.VMEM),
        cost_estimate=kernel_cost(2**19, 2**19, 2**12),
        name="incoming_state",
    )(here, joined, states)


def mix_kernel(within_ref, carry_q_ref, state_ref, gate_ref, gain_ref, out_ref):
    retained = within_ref[...] + dot(carry_q_ref[...], state_ref[...].astype(BF16))
    center = jnp.mean(retained, axis=-1, keepdims=True)
    off = retained - center
    spread = jnp.mean(off * off, axis=-1, keepdims=True)
    normed = off * lax.rsqrt(spread + EPS) * gain_ref[...].astype(F32)
    gate = gate_ref[...].astype(F32)
    mixed = (gate * jax.nn.sigmoid(gate) * normed).astype(BF16)
    places, cores, blocks, lines, _ = out_ref.shape
    for core in range(cores):
        for n in range(blocks):
            first = (n * cores + core) * lines
            piece = mixed[first : first + lines]
            for place in range(places):
                out_ref[place, core, n] = piece


def mix(within, carry_q, state, gate, gain):
    rows, width = within.shape
    return pl.pallas_call(
        mix_kernel,
        out_shape=jax.ShapeDtypeStruct((8, 2, 4, rows // 8, width), BF16),
        in_specs=vmem(5),
        out_specs=pl.BlockSpec(memory_space=pltpu.VMEM),
        cost_estimate=kernel_cost(2 * rows * width * width, 2**20, rows * width),
        name="mix",
    )(within, carry_q, state, gate, gain)


def rows_kernel(
    here_ref, mixed_ref, near_w_ref, far_w_ref, near_s_ref, far_s_ref, gain_ref, normed_ref, own_ref, residual
):
    halves, _, blocks, lines, head_dim = mixed_ref.shape
    count, width = normed_ref.shape
    x, c, y0 = here_ref[0], here_ref[1], here_ref[2]

    def heads_of(core):
        return jnp.concatenate(
            [
                jnp.concatenate(
                    [mixed_ref[n, ((x + 4 - r) % 4) * 2 + core].reshape(count // halves, head_dim) for r in range(4)],
                    axis=1,
                )
                for n in range(halves)
            ],
            axis=0,
        )

    near, far = heads_of(c), heads_of(1 - c)
    step = width // 4
    squares = jnp.zeros((count, 1), F32)
    for n in range(4):
        span = slice(n * step, (n + 1) * step)
        rows = []
        for half in range(halves):
            for block in range(blocks):
                at = (x + 4 - block) % 4
                rows.append(jnp.where(y0 == half, near_s_ref[at, :, span], far_s_ref[at, :, span]))
        part = (
            jnp.concatenate(rows, axis=0).astype(F32)
            + dot(near, near_w_ref[:, span])
            + dot(far, far_w_ref[:, span])
        )
        residual[:, span] = part
        squares += jnp.sum(part * part, axis=-1, keepdims=True)
    factor = lax.rsqrt(squares / width + EPS)
    for n in range(4):
        span = slice(n * step, (n + 1) * step)
        normed_ref[:, span] = (residual[:, span] * factor * gain_ref[:, span].astype(F32)).astype(BF16)
    first = pl.multiple_of((y0 * blocks + x) * lines, lines)
    own_ref[...] = residual[pl.ds(first, lines), :]


def group_rows(here, mixed, near_w, far_w, near_s, far_s, gain):
    lines, width = near_s.shape[1:]
    count = 8 * lines
    return pl.pallas_call(
        rows_kernel,
        out_shape=(
            jax.ShapeDtypeStruct((count, width), BF16),
            jax.ShapeDtypeStruct((lines, width), F32),
        ),
        in_specs=[pl.BlockSpec(memory_space=pltpu.SMEM)] + vmem(6),
        out_specs=vmem(2),
        scratch_shapes=[pltpu.VMEM((count, width), F32)],
        cost_estimate=kernel_cost(2 * count * width * 1024, 2**23),
        name="group_rows",
    )(here, mixed, near_w, far_w, near_s, far_s, gain)


CHUNKS = 4


def ffn_kernel(rows_ref, weight_ref, out_ref, held, sems):
    z, _, _, _, lines, hidden_width = weight_ref.shape
    each = z // CHUNKS
    depth = each * 4 * lines

    def copies(kind, n):
        span = pl.ds(n * each, each)
        return [
            pltpu.make_async_copy(
                weight_ref.at[span, y0, y1, kind],
                held.at[kind, span, y1, y0],
                sems.at[kind, n, 2 * y1 + y0],
            )
            for y1 in range(2)
            for y0 in range(2)
        ]

    for n in range(CHUNKS):
        for kind in (0, 1):
            for copy in copies(kind, n):
                copy.start()
    for n in range(CHUNKS):
        for copy in copies(2, n):
            copy.start()

    def block(kind, n):
        return held[kind, n * each : (n + 1) * each].reshape(depth, hidden_width)

    gate_sum = up_sum = None
    for n in range(CHUNKS):
        for kind in (0, 1):
            for copy in copies(kind, n):
                copy.wait()
        rows = rows_ref[:, n * depth : (n + 1) * depth]
        gate_part, up_part = dot(rows, block(0, n)), dot(rows, block(1, n))
        gate_sum = gate_part if gate_sum is None else gate_sum + gate_part
        up_sum = up_part if up_sum is None else up_sum + up_part
    hidden = (gate_sum * jax.nn.sigmoid(gate_sum) * up_sum).astype(BF16)
    for n in range(CHUNKS):
        for copy in copies(2, n):
            copy.wait()
        out_ref[:, n * depth : (n + 1) * depth] = dot_nt(hidden, block(2, n)).astype(BF16)


def feed_forward(rows, weights):
    count, width = rows.shape
    z, y0, y1, kinds, lines, hidden_width = weights.shape
    return pl.pallas_call(
        ffn_kernel,
        out_shape=jax.ShapeDtypeStruct((count, width), BF16),
        in_specs=[
            pl.BlockSpec(memory_space=pltpu.VMEM),
            pl.BlockSpec(memory_space=pl.ANY),
        ],
        out_specs=pl.BlockSpec(memory_space=pltpu.VMEM),
        scratch_shapes=[
            pltpu.VMEM((kinds, z, y1, y0, lines, hidden_width), BF16),
            pltpu.SemaphoreType.DMA((kinds, CHUNKS, 4)),
        ],
        cost_estimate=kernel_cost(6 * count * width * hidden_width, 2**23, count * hidden_width),
        name="feed_forward",
    )(rows, weights)


def moved(value, axes, place):
    lengths = [SIZES[a] for a in axes]
    pairs = []
    for y1 in range(lengths[0]):
        for y0 in range(lengths[1]):
            for c in range(lengths[2]):
                a, b, d = place(y1, y0, c)
                pairs.append(((y1 * 2 + y0) * 2 + c, (a * 2 + b) * 2 + d))
    return lax.ppermute(value, axes, pairs)


def shifted(value, axis, by):
    length = SIZES[axis]
    return lax.ppermute(value, axis, [(i, (i + by) % length) for i in range(length)])


def exchange(tiles, axes):
    return lax.all_to_all(tiles, axes, split_axis=0, concat_axis=0, tiled=True)


def gathered_weights(gate_weight, up_weight, down_weight):
    mine = jnp.concatenate([gate_weight, up_weight, down_weight.T], axis=0)
    lines, width = mine.shape
    axes = ("y1", "y0", "c")
    near = moved(mine, axes, lambda y1, y0, c: (y1, c, y0))
    far = moved(mine, axes, lambda y1, y0, c: (1 - y1, c, y0))
    upper = lax.axis_index("y1") == 1
    pair = jnp.stack([jnp.where(upper, far, near), jnp.where(upper, near, far)])
    whole = lax.all_gather(pair, Z + ("c",), axis=0)
    return whole.reshape(16, 2, 2, 3, lines // 3, width)


def layer(
    stream,
    queries,
    keys_in,
    values_in,
    gate_in,
    log_decay,
    head_gain,
    out_weight,
    norm_gain,
    gate_weight,
    up_weight,
    down_weight,
):
    weights = gathered_weights(gate_weight, up_weight, down_weight)
    rows, width = queries.shape[0], stream.shape[1]
    head_dim = queries.shape[1]
    block = jnp.concatenate([out_weight, stream], axis=0)
    found = [block] + [shifted(block, "x", r) for r in (1, 2, 3)]
    near_w = jnp.concatenate([b[:head_dim] for b in found], axis=0)
    near_s = jnp.stack([b[head_dim:] for b in found])
    far_w = shifted(near_w, "c", 1)
    far_s = shifted(near_s, "y0", 1)
    within, carry_q, state = retention(
        queries, keys_in, values_in, log_decay.reshape(1, rows)
    )
    states = exchange(state, NEAR)
    joined = joined_state(states)
    joined = exchange(joined, "zh")
    zh = lax.axis_index("zh").astype(jnp.int32).reshape(1)
    entering = incoming_state(zh, joined, states)
    entering = exchange(entering, NEAR)
    entering = entering.reshape(head_dim, head_dim)
    sent = mix(within, carry_q, entering, gate_in, head_gain.reshape(1, -1))
    mixed = exchange(sent.reshape(16, *sent.shape[2:]), GROUP + ("c",))
    here = jnp.stack([lax.axis_index(a).astype(jnp.int32) for a in ("x", "c", "y0")])
    normed, residual = group_rows(
        here, mixed.reshape(2, 8, *mixed.shape[1:]), near_w, far_w, near_s, far_s, norm_gain.reshape(1, -1)
    )
    down_terms = feed_forward(normed, weights)
    mixer_out = exchange(down_terms.reshape(8, rows // 8, width), GROUP).astype(F32).sum(axis=0)
    return (residual + mixer_out).astype(BF16)


def solution(mesh):
    finer = Mesh(mesh.devices.reshape(*SIZES.values()), tuple(SIZES))
    return jax.shard_map(
        layer,
        mesh=finer,
        in_specs=(
            P(SP + TP, None),
            P(SP, TP),
            P(SP, TP),
            P(SP, TP),
            P(SP, TP),
            P(SP, TP),
            P(TP),
            P(TP, None),
            P(),
            P(SP, TP),
            P(SP, TP),
            P(TP, SP),
        ),
        out_specs=P(SP + TP, None),
        check_vma=False,
    )
```

```python
import jax
import jax.numpy as jnp
from jax import lax
from jax.experimental import pallas as pl
from jax.experimental.pallas import tpu as pltpu
from jax.sharding import Mesh
from jax.sharding import PartitionSpec as P


Z, Y = ("zh", "zl"), ("y1", "y0")
NEAR = ("zl",) + Y
SP = Z + Y
TP = ("x", "c")
GROUP = ("y0", "x")
SIZES = {"zh": 4, "zl": 4, "y1": 2, "y0": 2, "x": 4, "c": 2}
EPS = 1e-6
F32, BF16 = jnp.float32, jnp.bfloat16


def vmem(count):
    return [pl.BlockSpec(memory_space=pltpu.VMEM)] * count


def kernel_cost(flops, moved, exps=0):
    return pl.CostEstimate(flops=flops, bytes_accessed=moved, transcendentals=exps)


def dot(a, b):
    return jnp.dot(a, b, preferred_element_type=F32)


def dot_nt(a, b):
    return lax.dot_general(a, b, (((1,), (1,)), ((), ())), preferred_element_type=F32)


def dot_tn(a, b):
    return lax.dot_general(a, b, (((0,), (0,)), ((), ())), preferred_element_type=F32)


def retention_kernel(q_ref, k_ref, v_ref, decay_ref, within_ref, carry_q_ref, state_ref):
    rows, head_dim = q_ref.shape
    scale = head_dim**-0.5
    at = lax.broadcasted_iota(jnp.int32, (rows, rows), 0)
    to = lax.broadcasted_iota(jnp.int32, (rows, rows), 1)
    causal = at >= to
    running = jnp.sum(jnp.where(causal, decay_ref[...], 0.0), axis=1, keepdims=True)
    across = jnp.sum(jnp.where(at == to, running, 0.0), axis=0, keepdims=True)
    total = running[rows - 1 : rows, :]
    q, k, v = q_ref[...], k_ref[...], v_ref[...]
    table = jnp.where(causal, jnp.exp(jnp.minimum(running - across, 0.0)), 0.0)
    scores = dot_nt(q, k) * scale
    within_ref[...] = dot((scores * table).astype(BF16), v)
    carry_q_ref[...] = (q.astype(F32) * jnp.exp(running)).astype(BF16)
    key_wide = (k.astype(F32) * scale * jnp.exp(total - running)).astype(BF16)
    state = dot_tn(key_wide, v)
    fill = jnp.broadcast_to(total, (8, head_dim))
    slices = state_ref.shape[0]
    part = head_dim // slices
    for n in range(slices):
        state_ref[n, :part, :] = state[n * part : (n + 1) * part]
        state_ref[n, part:, :] = fill


def retention(q, k, v, decay):
    rows, head_dim = q.shape
    part = head_dim // 16
    return pl.pallas_call(
        retention_kernel,
        out_shape=(
            jax.ShapeDtypeStruct((rows, head_dim), F32),
            jax.ShapeDtypeStruct((rows, head_dim), BF16),
            jax.ShapeDtypeStruct((16, part + 8, head_dim), F32),
        ),
        in_specs=vmem(4),
        out_specs=vmem(3),
        cost_estimate=kernel_cost(6 * rows * rows * head_dim, 2**20, rows * rows),
        name="retention",
    )(q, k, v, decay)


def joined_kernel(states_ref, out_ref):
    part = states_ref.shape[1] - 8
    state = states_ref[0, :part, :]
    total = states_ref[0, part:, :]
    for n in range(1, states_ref.shape[0]):
        own = states_ref[n, part:, :]
        state = jnp.exp(own) * state + states_ref[n, :part, :]
        total = total + own
    for n in range(out_ref.shape[0]):
        out_ref[n, :part, :] = state
        out_ref[n, part:, :] = total


def joined_state(states):
    _, lines, width = states.shape
    return pl.pallas_call(
        joined_kernel,
        out_shape=jax.ShapeDtypeStruct((4, lines, width), F32),
        in_specs=vmem(1),
        out_specs=pl.BlockSpec(memory_space=pltpu.VMEM),
        cost_estimate=kernel_cost(2**18, 2**18, 2**10),
        compiler_params=pltpu.CompilerParams(vmem_limit_bytes=2 * 2**20),
        name="joined_state",
    )(states)


def incoming_kernel(here_ref, joined_ref, states_ref, out_ref):
    part = out_ref.shape[1]
    here = here_ref[0]
    carried = jnp.zeros(out_ref.shape[1:], F32)
    for n in range(joined_ref.shape[0]):
        after = jnp.exp(joined_ref[n, part:, :]) * carried + joined_ref[n, :part, :]
        carried = jnp.where(n < here, after, carried)
    for n in range(out_ref.shape[0]):
        out_ref[n] = carried
        carried = jnp.exp(states_ref[n, part:, :]) * carried + states_ref[n, :part, :]


def incoming_state(here, joined, states):
    count, lines, width = states.shape
    return pl.pallas_call(
        incoming_kernel,
        out_shape=jax.ShapeDtypeStruct((count, lines - 8, width), F32),
        in_specs=[pl.BlockSpec(memory_space=pltpu.SMEM)] + vmem(2),
        out_specs=pl.BlockSpec(memory_space=pltpu.VMEM),
        cost_estimate=kernel_cost(2**19, 2**19, 2**12),
        compiler_params=pltpu.CompilerParams(vmem_limit_bytes=2 * 2**20),
        name="incoming_state",
    )(here, joined, states)


def mix_kernel(within_ref, carry_q_ref, state_ref, gate_ref, gain_ref, out_ref):
    retained = within_ref[...] + dot(carry_q_ref[...], state_ref[...].astype(BF16))
    center = jnp.mean(retained, axis=-1, keepdims=True)
    off = retained - center
    spread = jnp.mean(off * off, axis=-1, keepdims=True)
    normed = off * lax.rsqrt(spread + EPS) * gain_ref[...].astype(F32)
    gate = gate_ref[...].astype(F32)
    mixed = (gate * jax.nn.sigmoid(gate) * normed).astype(BF16)
    places, cores, blocks, lines, _ = out_ref.shape
    for core in range(cores):
        for n in range(blocks):
            first = (n * cores + core) * lines
            piece = mixed[first : first + lines]
            for place in range(places):
                out_ref[place, core, n] = piece


def mix(within, carry_q, state, gate, gain):
    rows, width = within.shape
    return pl.pallas_call(
        mix_kernel,
        out_shape=jax.ShapeDtypeStruct((8, 2, 4, rows // 8, width), BF16),
        in_specs=vmem(5),
        out_specs=pl.BlockSpec(memory_space=pltpu.VMEM),
        cost_estimate=kernel_cost(2 * rows * width * width, 2**20, rows * width),
        name="mix",
    )(within, carry_q, state, gate, gain)


def rows_kernel(
    here_ref, mixed_ref, near_w_ref, far_w_ref, near_s_ref, far_s_ref, gain_ref, normed_ref, own_ref, residual
):
    halves, _, blocks, lines, head_dim = mixed_ref.shape
    count, width = normed_ref.shape
    x, c, y0 = here_ref[0], here_ref[1], here_ref[2]

    def heads_of(core):
        return jnp.concatenate(
            [
                jnp.concatenate(
                    [mixed_ref[n, ((x + 4 - r) % 4) * 2 + core].reshape(count // halves, head_dim) for r in range(4)],
                    axis=1,
                )
                for n in range(halves)
            ],
            axis=0,
        )

    near, far = heads_of(c), heads_of(1 - c)
    step = width // 4
    squares = jnp.zeros((count, 1), F32)
    for n in range(4):
        span = slice(n * step, (n + 1) * step)
        rows = []
        for half in range(halves):
            for block in range(blocks):
                at = (x + 4 - block) % 4
                rows.append(jnp.where(y0 == half, near_s_ref[at, :, span], far_s_ref[at, :, span]))
        part = (
            jnp.concatenate(rows, axis=0).astype(F32)
            + dot(near, near_w_ref[:, span])
            + dot(far, far_w_ref[:, span])
        )
        residual[:, span] = part
        squares += jnp.sum(part * part, axis=-1, keepdims=True)
    factor = lax.rsqrt(squares / width + EPS)
    for n in range(4):
        span = slice(n * step, (n + 1) * step)
        normed_ref[:, span] = (residual[:, span] * factor * gain_ref[:, span].astype(F32)).astype(BF16)
    first = pl.multiple_of((y0 * blocks + x) * lines, lines)
    own_ref[...] = residual[pl.ds(first, lines), :]


def group_rows(here, mixed, near_w, far_w, near_s, far_s, gain):
    lines, width = near_s.shape[1:]
    count = 8 * lines
    return pl.pallas_call(
        rows_kernel,
        out_shape=(
            jax.ShapeDtypeStruct((count, width), BF16),
            jax.ShapeDtypeStruct((lines, width), F32),
        ),
        in_specs=[pl.BlockSpec(memory_space=pltpu.SMEM)] + vmem(6),
        out_specs=vmem(2),
        scratch_shapes=[pltpu.VMEM((count, width), F32)],
        cost_estimate=kernel_cost(2 * count * width * 1024, 2**23),
        compiler_params=pltpu.CompilerParams(vmem_limit_bytes=20 * 2**20),
        name="group_rows",
    )(here, mixed, near_w, far_w, near_s, far_s, gain)


CHUNKS = 4


def ffn_kernel(rows_ref, weight_ref, out_ref, held, sems):
    z, _, _, _, lines, hidden_width = weight_ref.shape
    each = z // CHUNKS
    depth = each * 4 * lines

    def copies(kind, n):
        span = pl.ds(n * each, each)
        return [
            pltpu.make_async_copy(
                weight_ref.at[span, y0, y1, kind],
                held.at[kind, span, y1, y0],
                sems.at[kind, n, 2 * y1 + y0],
            )
            for y1 in range(2)
            for y0 in range(2)
        ]

    for n in range(CHUNKS):
        for kind in (0, 1):
            for copy in copies(kind, n):
                copy.start()
    for n in range(CHUNKS):
        for copy in copies(2, n):
            copy.start()

    def block(kind, n):
        return held[kind, n * each : (n + 1) * each].reshape(depth, hidden_width)

    gate_sum = up_sum = None
    for n in range(CHUNKS):
        for kind in (0, 1):
            for copy in copies(kind, n):
                copy.wait()
        rows = rows_ref[:, n * depth : (n + 1) * depth]
        gate_part, up_part = dot(rows, block(0, n)), dot(rows, block(1, n))
        gate_sum = gate_part if gate_sum is None else gate_sum + gate_part
        up_sum = up_part if up_sum is None else up_sum + up_part
    hidden = (gate_sum * jax.nn.sigmoid(gate_sum) * up_sum).astype(BF16)
    for n in range(CHUNKS):
        for copy in copies(2, n):
            copy.wait()
        out_ref[:, n * depth : (n + 1) * depth] = dot_nt(hidden, block(2, n)).astype(BF16)


def feed_forward(rows, weights):
    count, width = rows.shape
    z, y0, y1, kinds, lines, hidden_width = weights.shape
    return pl.pallas_call(
        ffn_kernel,
        out_shape=jax.ShapeDtypeStruct((count, width), BF16),
        in_specs=[
            pl.BlockSpec(memory_space=pltpu.VMEM),
            pl.BlockSpec(memory_space=pl.ANY),
        ],
        out_specs=pl.BlockSpec(memory_space=pltpu.VMEM),
        scratch_shapes=[
            pltpu.VMEM((kinds, z, y1, y0, lines, hidden_width), BF16),
            pltpu.SemaphoreType.DMA((kinds, CHUNKS, 4)),
        ],
        cost_estimate=kernel_cost(6 * count * width * hidden_width, 2**23, count * hidden_width),
        compiler_params=pltpu.CompilerParams(vmem_limit_bytes=56 * 2**20),
        name="feed_forward",
    )(rows, weights)


def moved(value, axes, place):
    lengths = [SIZES[a] for a in axes]
    pairs = []
    for y1 in range(lengths[0]):
        for y0 in range(lengths[1]):
            for c in range(lengths[2]):
                a, b, d = place(y1, y0, c)
                pairs.append(((y1 * 2 + y0) * 2 + c, (a * 2 + b) * 2 + d))
    return lax.ppermute(value, axes, pairs)


def shifted(value, axis, by):
    length = SIZES[axis]
    return lax.ppermute(value, axis, [(i, (i + by) % length) for i in range(length)])


def exchange(tiles, axes):
    return lax.all_to_all(tiles, axes, split_axis=0, concat_axis=0, tiled=True)


def gathered_weights(gate_weight, up_weight, down_weight):
    mine = jnp.concatenate([gate_weight, up_weight, down_weight.T], axis=0)
    lines, width = mine.shape
    axes = ("y1", "y0", "c")
    near = moved(mine, axes, lambda y1, y0, c: (y1, c, y0))
    far = moved(mine, axes, lambda y1, y0, c: (1 - y1, c, y0))
    upper = lax.axis_index("y1") == 1
    pair = jnp.stack([jnp.where(upper, far, near), jnp.where(upper, near, far)])
    whole = lax.all_gather(pair, Z + ("c",), axis=0)
    return whole.reshape(16, 2, 2, 3, lines // 3, width)


def layer(
    stream,
    queries,
    keys_in,
    values_in,
    gate_in,
    log_decay,
    head_gain,
    out_weight,
    norm_gain,
    gate_weight,
    up_weight,
    down_weight,
):
    weights = gathered_weights(gate_weight, up_weight, down_weight)
    rows, width = queries.shape[0], stream.shape[1]
    head_dim = queries.shape[1]
    sides = [shifted(out_weight, "x", 1), shifted(out_weight, "x", 3)]
    across = shifted(out_weight, "x", 2)
    others = [shifted(stream, "x", r) for r in (1, 2, 3)]
    near_w = jnp.concatenate([out_weight, sides[0], across, sides[1]], axis=0)
    near_s = jnp.stack([stream, *others])
    far_w = shifted(near_w, "c", 1)
    far_s = shifted(near_s, "y0", 1)
    within, carry_q, state = retention(
        queries, keys_in, values_in, log_decay.reshape(1, rows)
    )
    states = exchange(state, NEAR)
    joined = joined_state(states)
    joined = exchange(joined, "zh")
    zh = lax.axis_index("zh").astype(jnp.int32).reshape(1)
    entering = incoming_state(zh, joined, states)
    entering = exchange(entering, NEAR)
    entering = entering.reshape(head_dim, head_dim)
    sent = mix(within, carry_q, entering, gate_in, head_gain.reshape(1, -1))
    mixed = exchange(sent.reshape(16, *sent.shape[2:]), GROUP + ("c",))
    here = jnp.stack([lax.axis_index(a).astype(jnp.int32) for a in ("x", "c", "y0")])
    normed, residual = group_rows(
        here, mixed.reshape(2, 8, *mixed.shape[1:]), near_w, far_w, near_s, far_s, norm_gain.reshape(1, -1)
    )
    down_terms = feed_forward(normed, weights)
    mixer_out = exchange(down_terms.reshape(8, rows // 8, width), GROUP).astype(F32).sum(axis=0)
    return (residual + mixer_out).astype(BF16)


def solution(mesh):
    finer = Mesh(mesh.devices.reshape(*SIZES.values()), tuple(SIZES))
    return jax.shard_map(
        layer,
        mesh=finer,
        in_specs=(
            P(SP + TP, None),
            P(SP, TP),
            P(SP, TP),
            P(SP, TP),
            P(SP, TP),
            P(SP, TP),
            P(TP),
            P(TP, None),
            P(),
            P(SP, TP),
            P(SP, TP),
            P(TP, SP),
        ),
        out_specs=P(SP + TP, None),
        check_vma=False,
    )
```

```python
import jax
import jax.numpy as jnp
from jax import lax
from jax.experimental import pallas as pl
from jax.experimental.pallas import tpu as pltpu
from jax.sharding import Mesh
from jax.sharding import PartitionSpec as P


Z, Y = ("zh", "zl"), ("y1", "y0")
NEAR = ("zl",) + Y
SP = Z + Y
TP = ("x", "c")
GROUP = ("y0", "x")
SIZES = {"zh": 4, "zl": 4, "y1": 2, "y0": 2, "x": 4, "c": 2}
EPS = 1e-6
F32, BF16 = jnp.float32, jnp.bfloat16


def vmem(count):
    return [pl.BlockSpec(memory_space=pltpu.VMEM)] * count


def kernel_cost(flops, moved, exps=0):
    return pl.CostEstimate(flops=flops, bytes_accessed=moved, transcendentals=exps)


def dot(a, b):
    return jnp.dot(a, b, preferred_element_type=F32)


def dot_nt(a, b):
    return lax.dot_general(a, b, (((1,), (1,)), ((), ())), preferred_element_type=F32)


def dot_tn(a, b):
    return lax.dot_general(a, b, (((0,), (0,)), ((), ())), preferred_element_type=F32)


def retention_kernel(q_ref, k_ref, v_ref, decay_ref, within_ref, carry_q_ref, state_ref):
    rows, head_dim = q_ref.shape
    scale = head_dim**-0.5
    at = lax.broadcasted_iota(jnp.int32, (rows, rows), 0)
    to = lax.broadcasted_iota(jnp.int32, (rows, rows), 1)
    causal = at >= to
    running = jnp.sum(jnp.where(causal, decay_ref[...], 0.0), axis=1, keepdims=True)
    across = jnp.sum(jnp.where(at == to, running, 0.0), axis=0, keepdims=True)
    total = running[rows - 1 : rows, :]
    q, k, v = q_ref[...], k_ref[...], v_ref[...]
    table = jnp.where(causal, jnp.exp(jnp.minimum(running - across, 0.0)), 0.0)
    scores = dot_nt(q, k) * scale
    within_ref[...] = dot((scores * table).astype(BF16), v)
    carry_q_ref[...] = (q.astype(F32) * jnp.exp(running)).astype(BF16)
    key_wide = (k.astype(F32) * scale * jnp.exp(total - running)).astype(BF16)
    state = dot_tn(key_wide, v)
    fill = jnp.broadcast_to(total, (8, head_dim))
    slices = state_ref.shape[0]
    part = head_dim // slices
    for n in range(slices):
        state_ref[n, :part, :] = state[n * part : (n + 1) * part]
        state_ref[n, part:, :] = fill


def retention(q, k, v, decay):
    rows, head_dim = q.shape
    part = head_dim // 16
    return pl.pallas_call(
        retention_kernel,
        out_shape=(
            jax.ShapeDtypeStruct((rows, head_dim), F32),
            jax.ShapeDtypeStruct((rows, head_dim), BF16),
            jax.ShapeDtypeStruct((16, part + 8, head_dim), F32),
        ),
        in_specs=vmem(4),
        out_specs=vmem(3),
        cost_estimate=kernel_cost(6 * rows * rows * head_dim, 2**20, rows * rows),
        name="retention",
    )(q, k, v, decay)


def joined_kernel(states_ref, out_ref):
    part = states_ref.shape[1] - 8
    state = states_ref[0, :part, :]
    total = states_ref[0, part:, :]
    for n in range(1, states_ref.shape[0]):
        own = states_ref[n, part:, :]
        state = jnp.exp(own) * state + states_ref[n, :part, :]
        total = total + own
    for n in range(out_ref.shape[0]):
        out_ref[n, :part, :] = state
        out_ref[n, part:, :] = total


def joined_state(states):
    _, lines, width = states.shape
    return pl.pallas_call(
        joined_kernel,
        out_shape=jax.ShapeDtypeStruct((4, lines, width), F32),
        in_specs=vmem(1),
        out_specs=pl.BlockSpec(memory_space=pltpu.VMEM),
        cost_estimate=kernel_cost(2**18, 2**18, 2**10),
        compiler_params=pltpu.CompilerParams(vmem_limit_bytes=2 * 2**20),
        name="joined_state",
    )(states)


def incoming_kernel(here_ref, joined_ref, states_ref, out_ref):
    part = out_ref.shape[1]
    here = here_ref[0]
    carried = jnp.zeros(out_ref.shape[1:], F32)
    for n in range(joined_ref.shape[0]):
        after = jnp.exp(joined_ref[n, part:, :]) * carried + joined_ref[n, :part, :]
        carried = jnp.where(n < here, after, carried)
    for n in range(out_ref.shape[0]):
        out_ref[n] = carried
        carried = jnp.exp(states_ref[n, part:, :]) * carried + states_ref[n, :part, :]


def incoming_state(here, joined, states):
    count, lines, width = states.shape
    return pl.pallas_call(
        incoming_kernel,
        out_shape=jax.ShapeDtypeStruct((count, lines - 8, width), F32),
        in_specs=[pl.BlockSpec(memory_space=pltpu.SMEM)] + vmem(2),
        out_specs=pl.BlockSpec(memory_space=pltpu.VMEM),
        cost_estimate=kernel_cost(2**19, 2**19, 2**12),
        compiler_params=pltpu.CompilerParams(vmem_limit_bytes=2 * 2**20),
        name="incoming_state",
    )(here, joined, states)


def mix_kernel(within_ref, carry_q_ref, state_ref, gate_ref, gain_ref, out_ref):
    retained = within_ref[...] + dot(carry_q_ref[...], state_ref[...].astype(BF16))
    center = jnp.mean(retained, axis=-1, keepdims=True)
    off = retained - center
    spread = jnp.mean(off * off, axis=-1, keepdims=True)
    normed = off * lax.rsqrt(spread + EPS) * gain_ref[...].astype(F32)
    gate = gate_ref[...].astype(F32)
    mixed = (gate * jax.nn.sigmoid(gate) * normed).astype(BF16)
    places, cores, blocks, lines, _ = out_ref.shape
    for core in range(cores):
        for n in range(blocks):
            first = (n * cores + core) * lines
            piece = mixed[first : first + lines]
            for place in range(places):
                out_ref[place, core, n] = piece


def mix(within, carry_q, state, gate, gain):
    rows, width = within.shape
    return pl.pallas_call(
        mix_kernel,
        out_shape=jax.ShapeDtypeStruct((8, 2, 4, rows // 8, width), BF16),
        in_specs=vmem(5),
        out_specs=pl.BlockSpec(memory_space=pltpu.VMEM),
        cost_estimate=kernel_cost(2 * rows * width * width, 2**20, rows * width),
        name="mix",
    )(within, carry_q, state, gate, gain)


def rows_kernel(
    here_ref, mixed_ref, near_w_ref, far_w_ref, near_s_ref, far_s_ref, gain_ref, normed_ref, own_ref, residual, normed, sems
):
    halves, _, blocks, lines, head_dim = mixed_ref.shape
    count, width = normed_ref.shape
    x, c, y0 = here_ref[0], here_ref[1], here_ref[2]

    def heads_of(core):
        return jnp.concatenate(
            [
                jnp.concatenate(
                    [mixed_ref[n, ((x + 4 - r) % 4) * 2 + core].reshape(count // halves, head_dim) for r in range(4)],
                    axis=1,
                )
                for n in range(halves)
            ],
            axis=0,
        )

    near, far = heads_of(c), heads_of(1 - c)
    step = width // 4
    squares = jnp.zeros((count, 1), F32)
    for n in range(4):
        span = slice(n * step, (n + 1) * step)
        rows = []
        for half in range(halves):
            for block in range(blocks):
                at = (x + 4 - block) % 4
                rows.append(jnp.where(y0 == half, near_s_ref[at, :, span], far_s_ref[at, :, span]))
        part = (
            jnp.concatenate(rows, axis=0).astype(F32)
            + dot(near, near_w_ref[:, span])
            + dot(far, far_w_ref[:, span])
        )
        residual[:, span] = part
        squares += jnp.sum(part * part, axis=-1, keepdims=True)
    factor = lax.rsqrt(squares / width + EPS)
    copies = []
    for n in range(4):
        span = slice(n * step, (n + 1) * step)
        normed[:, span] = (residual[:, span] * factor * gain_ref[:, span].astype(F32)).astype(BF16)
        copies.append(pltpu.make_async_copy(normed.at[:, span], normed_ref.at[:, span], sems.at[n]))
        copies[n].start()
    first = pl.multiple_of((y0 * blocks + x) * lines, lines)
    own_ref[...] = residual[pl.ds(first, lines), :]
    for copy in copies:
        copy.wait()


def group_rows(here, mixed, near_w, far_w, near_s, far_s, gain):
    lines, width = near_s.shape[1:]
    count = 8 * lines
    return pl.pallas_call(
        rows_kernel,
        out_shape=(
            jax.ShapeDtypeStruct((count, width), BF16),
            jax.ShapeDtypeStruct((lines, width), F32),
        ),
        in_specs=[pl.BlockSpec(memory_space=pltpu.SMEM)] + vmem(6),
        out_specs=[pl.BlockSpec(memory_space=pltpu.HBM)] + vmem(1),
        scratch_shapes=[
            pltpu.VMEM((count, width), F32),
            pltpu.VMEM((count, width), BF16),
            pltpu.SemaphoreType.DMA((4,)),
        ],
        cost_estimate=kernel_cost(2 * count * width * 1024, 2**23),
        compiler_params=pltpu.CompilerParams(vmem_limit_bytes=20 * 2**20),
        name="group_rows",
    )(here, mixed, near_w, far_w, near_s, far_s, gain)


CHUNKS = (2, 1, 1)


def ffn_kernel(rows_ref, weight_ref, out_ref, rows, held, rows_sem, sems):
    z, _, _, kinds, lines, hidden_width = weight_ref.shape

    def copies(kind, n):
        each = z // CHUNKS[kind]
        span = pl.ds(n * each, each)
        return [
            pltpu.make_async_copy(
                weight_ref.at[span, y0, y1, kind],
                held.at[kind, span, y1, y0],
                sems.at[kind, n, 2 * y1 + y0],
            )
            for y1 in range(2)
            for y0 in range(2)
        ]

    def arrived(kind, n):
        each = z // CHUNKS[kind]
        for copy in copies(kind, n):
            copy.wait()
        depth = each * 4 * lines
        return held[kind, n * each : (n + 1) * each].reshape(depth, hidden_width), depth

    fetch = pltpu.make_async_copy(rows_ref, rows, rows_sem)
    fetch.start()
    for kind in range(kinds):
        for n in range(CHUNKS[kind]):
            for copy in copies(kind, n):
                copy.start()
    fetch.wait()
    sums = []
    for kind in (0, 1):
        total = None
        for n in range(CHUNKS[kind]):
            block, depth = arrived(kind, n)
            part = dot(rows[:, n * depth : (n + 1) * depth], block)
            total = part if total is None else total + part
        sums.append(total)
    gate_sum, up_sum = sums
    hidden = (gate_sum * jax.nn.sigmoid(gate_sum) * up_sum).astype(BF16)
    for n in range(CHUNKS[2]):
        block, depth = arrived(2, n)
        out_ref[:, n * depth : (n + 1) * depth] = dot_nt(hidden, block).astype(BF16)


def feed_forward(rows, weights):
    count, width = rows.shape
    z, y0, y1, kinds, lines, hidden_width = weights.shape
    return pl.pallas_call(
        ffn_kernel,
        out_shape=jax.ShapeDtypeStruct((count, width), BF16),
        in_specs=[pl.BlockSpec(memory_space=pltpu.HBM)] * 2,
        out_specs=pl.BlockSpec(memory_space=pltpu.VMEM),
        scratch_shapes=[
            pltpu.VMEM((count, width), BF16),
            pltpu.VMEM((kinds, z, y1, y0, lines, hidden_width), BF16),
            pltpu.SemaphoreType.DMA,
            pltpu.SemaphoreType.DMA((kinds, max(CHUNKS), 4)),
        ],
        cost_estimate=kernel_cost(6 * count * width * hidden_width, 2**23, count * hidden_width),
        compiler_params=pltpu.CompilerParams(vmem_limit_bytes=52 * 2**20),
        name="feed_forward",
    )(rows, weights)


def moved(value, axes, place):
    lengths = [SIZES[a] for a in axes]
    pairs = []
    for y1 in range(lengths[0]):
        for y0 in range(lengths[1]):
            for c in range(lengths[2]):
                a, b, d = place(y1, y0, c)
                pairs.append(((y1 * 2 + y0) * 2 + c, (a * 2 + b) * 2 + d))
    return lax.ppermute(value, axes, pairs)


def shifted(value, axis, by):
    length = SIZES[axis]
    return lax.ppermute(value, axis, [(i, (i + by) % length) for i in range(length)])


def exchange(tiles, axes):
    return lax.all_to_all(tiles, axes, split_axis=0, concat_axis=0, tiled=True)


def gathered_weights(gate_weight, up_weight, down_weight):
    mine = jnp.concatenate([gate_weight, up_weight, down_weight.T], axis=0)
    lines, width = mine.shape
    axes = ("y1", "y0", "c")
    near = moved(mine, axes, lambda y1, y0, c: (y1, c, y0))
    far = moved(mine, axes, lambda y1, y0, c: (1 - y1, c, y0))
    upper = lax.axis_index("y1") == 1
    pair = jnp.stack([jnp.where(upper, far, near), jnp.where(upper, near, far)])
    whole = lax.all_gather(pair, Z + ("c",), axis=0)
    return whole.reshape(16, 2, 2, 3, lines // 3, width)


def layer(
    stream,
    queries,
    keys_in,
    values_in,
    gate_in,
    log_decay,
    head_gain,
    out_weight,
    norm_gain,
    gate_weight,
    up_weight,
    down_weight,
):
    weights = gathered_weights(gate_weight, up_weight, down_weight)
    rows, width = queries.shape[0], stream.shape[1]
    head_dim = queries.shape[1]
    sides = [shifted(out_weight, "x", 1), shifted(out_weight, "x", 3)]
    across = shifted(out_weight, "x", 2)
    others = [shifted(stream, "x", r) for r in (1, 2, 3)]
    near_w = jnp.concatenate([out_weight, sides[0], across, sides[1]], axis=0)
    near_s = jnp.stack([stream, *others])
    far_w = shifted(near_w, "c", 1)
    far_s = shifted(near_s, "y0", 1)
    within, carry_q, state = retention(
        queries, keys_in, values_in, log_decay.reshape(1, rows)
    )
    states = exchange(state, NEAR)
    joined = joined_state(states)
    joined = exchange(joined, "zh")
    zh = lax.axis_index("zh").astype(jnp.int32).reshape(1)
    entering = incoming_state(zh, joined, states)
    entering = exchange(entering, NEAR)
    entering = entering.reshape(head_dim, head_dim)
    sent = mix(within, carry_q, entering, gate_in, head_gain.reshape(1, -1))
    mixed = exchange(sent.reshape(16, *sent.shape[2:]), GROUP + ("c",))
    here = jnp.stack([lax.axis_index(a).astype(jnp.int32) for a in ("x", "c", "y0")])
    normed, residual = group_rows(
        here, mixed.reshape(2, 8, *mixed.shape[1:]), near_w, far_w, near_s, far_s, norm_gain.reshape(1, -1)
    )
    down_terms = feed_forward(normed, weights)
    mixer_out = exchange(down_terms.reshape(8, rows // 8, width), GROUP).astype(F32).sum(axis=0)
    return (residual + mixer_out).astype(BF16)


def solution(mesh):
    finer = Mesh(mesh.devices.reshape(*SIZES.values()), tuple(SIZES))
    return jax.shard_map(
        layer,
        mesh=finer,
        in_specs=(
            P(SP + TP, None),
            P(SP, TP),
            P(SP, TP),
            P(SP, TP),
            P(SP, TP),
            P(SP, TP),
            P(TP),
            P(TP, None),
            P(),
            P(SP, TP),
            P(SP, TP),
            P(TP, SP),
        ),
        out_specs=P(SP + TP, None),
        check_vma=False,
    )
```

```python
import jax
import jax.numpy as jnp
from jax import lax
from jax.experimental import pallas as pl
from jax.experimental.pallas import tpu as pltpu
from jax.sharding import Mesh
from jax.sharding import PartitionSpec as P


Z, Y = ("zh", "zl"), ("y1", "y0")
NEAR = ("zl",) + Y
SP = Z + Y
TP = ("x", "c")
GROUP = ("y0", "x")
SIZES = {"zh": 8, "zl": 2, "y1": 2, "y0": 2, "x": 4, "c": 2}
EPS = 1e-6
NEIGHBOURS = 8
F32, BF16 = jnp.float32, jnp.bfloat16


def vmem(count):
    return [pl.BlockSpec(memory_space=pltpu.VMEM)] * count


def kernel_cost(flops, moved, exps=0):
    return pl.CostEstimate(flops=flops, bytes_accessed=moved, transcendentals=exps)


def dot(a, b):
    return jnp.dot(a, b, preferred_element_type=F32)


def dot_nt(a, b):
    return lax.dot_general(a, b, (((1,), (1,)), ((), ())), preferred_element_type=F32)


def dot_tn(a, b):
    return lax.dot_general(a, b, (((0,), (0,)), ((), ())), preferred_element_type=F32)


def retention_kernel(q_ref, k_ref, v_ref, decay_ref, within_ref, carry_q_ref, state_ref):
    rows, head_dim = q_ref.shape
    scale = head_dim**-0.5
    at = lax.broadcasted_iota(jnp.int32, (rows, rows), 0)
    to = lax.broadcasted_iota(jnp.int32, (rows, rows), 1)
    causal = at >= to
    running = jnp.sum(jnp.where(causal, decay_ref[...], 0.0), axis=1, keepdims=True)
    across = jnp.sum(jnp.where(at == to, running, 0.0), axis=0, keepdims=True)
    total = running[rows - 1 : rows, :]
    q, k, v = q_ref[...], k_ref[...], v_ref[...]
    table = jnp.where(causal, jnp.exp(jnp.minimum(running - across, 0.0)), 0.0)
    scores = dot_nt(q, k) * scale
    within_ref[...] = dot((scores * table).astype(BF16), v)
    carry_q_ref[...] = (q.astype(F32) * jnp.exp(running)).astype(BF16)
    key_wide = (k.astype(F32) * scale * jnp.exp(total - running)).astype(BF16)
    state = dot_tn(key_wide, v)
    fill = jnp.broadcast_to(total, (8, head_dim))
    slices = state_ref.shape[0]
    part = head_dim // slices
    for n in range(slices):
        state_ref[n, :part, :] = state[n * part : (n + 1) * part]
        state_ref[n, part:, :] = fill


def retention(q, k, v, decay):
    rows, head_dim = q.shape
    part = head_dim // NEIGHBOURS
    return pl.pallas_call(
        retention_kernel,
        out_shape=(
            jax.ShapeDtypeStruct((rows, head_dim), F32),
            jax.ShapeDtypeStruct((rows, head_dim), BF16),
            jax.ShapeDtypeStruct((NEIGHBOURS, part + 8, head_dim), F32),
        ),
        in_specs=vmem(4),
        out_specs=vmem(3),
        cost_estimate=kernel_cost(6 * rows * rows * head_dim, 2**20, rows * rows),
        name="retention",
    )(q, k, v, decay)


def joined_kernel(states_ref, out_ref):
    part = states_ref.shape[1] - 8
    state = states_ref[0, :part, :]
    total = states_ref[0, part:, :]
    for n in range(1, states_ref.shape[0]):
        own = states_ref[n, part:, :]
        state = jnp.exp(own[:1]) * state + states_ref[n, :part, :]
        total = total + own
    for n in range(out_ref.shape[0]):
        out_ref[n, :part, :] = state
        out_ref[n, part:, :] = total


def joined_state(states):
    _, lines, width = states.shape
    return pl.pallas_call(
        joined_kernel,
        out_shape=jax.ShapeDtypeStruct((SIZES["zh"], lines, width), F32),
        in_specs=vmem(1),
        out_specs=pl.BlockSpec(memory_space=pltpu.VMEM),
        cost_estimate=kernel_cost(2**18, 2**18, 2**10),
        compiler_params=pltpu.CompilerParams(vmem_limit_bytes=2 * 2**20),
        name="joined_state",
    )(states)


def incoming_kernel(here_ref, joined_ref, states_ref, out_ref):
    part = out_ref.shape[1]
    here = here_ref[0]
    carried = jnp.zeros(out_ref.shape[1:], F32)
    for n in range(joined_ref.shape[0]):
        after = jnp.exp(joined_ref[n, part : part + 1, :]) * carried + joined_ref[n, :part, :]
        carried = jnp.where(n < here, after, carried)
    for n in range(out_ref.shape[0]):
        out_ref[n] = carried
        carried = jnp.exp(states_ref[n, part : part + 1, :]) * carried + states_ref[n, :part, :]


def incoming_state(here, joined, states):
    count, lines, width = states.shape
    return pl.pallas_call(
        incoming_kernel,
        out_shape=jax.ShapeDtypeStruct((count, lines - 8, width), F32),
        in_specs=[pl.BlockSpec(memory_space=pltpu.SMEM)] + vmem(2),
        out_specs=pl.BlockSpec(memory_space=pltpu.VMEM),
        cost_estimate=kernel_cost(2**19, 2**19, 2**12),
        compiler_params=pltpu.CompilerParams(vmem_limit_bytes=2 * 2**20),
        name="incoming_state",
    )(here, joined, states)


def mix_kernel(within_ref, carry_q_ref, state_ref, gate_ref, gain_ref, out_ref):
    retained = within_ref[...] + dot(carry_q_ref[...], state_ref[...].astype(BF16))
    center = jnp.mean(retained, axis=-1, keepdims=True)
    off = retained - center
    spread = jnp.mean(off * off, axis=-1, keepdims=True)
    normed = off * lax.rsqrt(spread + EPS) * gain_ref[...].astype(F32)
    gate = gate_ref[...].astype(F32)
    mixed = (gate * jax.nn.sigmoid(gate) * normed).astype(BF16)
    places, cores, blocks, lines, _ = out_ref.shape
    for core in range(cores):
        for n in range(blocks):
            first = (n * cores + core) * lines
            piece = mixed[first : first + lines]
            for place in range(places):
                out_ref[place, core, n] = piece


def mix(within, carry_q, state, gate, gain):
    rows, width = within.shape
    return pl.pallas_call(
        mix_kernel,
        out_shape=jax.ShapeDtypeStruct((8, 2, 4, rows // 8, width), BF16),
        in_specs=vmem(5),
        out_specs=pl.BlockSpec(memory_space=pltpu.VMEM),
        cost_estimate=kernel_cost(2 * rows * width * width, 2**20, rows * width),
        name="mix",
    )(within, carry_q, state, gate, gain)


def rows_kernel(
    here_ref, mixed_ref, near_w_ref, far_w_ref, near_s_ref, far_s_ref, gain_ref, normed_ref, own_ref, residual, normed, sems
):
    halves, _, blocks, lines, head_dim = mixed_ref.shape
    count, width = normed_ref.shape
    x, c, y0 = here_ref[0], here_ref[1], here_ref[2]

    def heads_of(core):
        return jnp.concatenate(
            [
                jnp.concatenate(
                    [mixed_ref[n, ((x + 4 - r) % 4) * 2 + core].reshape(count // halves, head_dim) for r in range(4)],
                    axis=1,
                )
                for n in range(halves)
            ],
            axis=0,
        )

    near, far = heads_of(c), heads_of(1 - c)
    step = width // 4
    squares = jnp.zeros((count, 1), F32)
    for n in range(4):
        span = slice(n * step, (n + 1) * step)
        rows = []
        for half in range(halves):
            for block in range(blocks):
                at = (x + 4 - block) % 4
                rows.append(jnp.where(y0 == half, near_s_ref[at, :, span], far_s_ref[at, :, span]))
        part = (
            jnp.concatenate(rows, axis=0).astype(F32)
            + dot(near, near_w_ref[:, span])
            + dot(far, far_w_ref[:, span])
        )
        residual[:, span] = part
        squares += jnp.sum(part * part, axis=-1, keepdims=True)
    factor = lax.rsqrt(squares / width + EPS)
    copies = []
    for n in range(4):
        span = slice(n * step, (n + 1) * step)
        normed[:, span] = (residual[:, span] * factor * gain_ref[:, span].astype(F32)).astype(BF16)
        copies.append(pltpu.make_async_copy(normed.at[:, span], normed_ref.at[:, span], sems.at[n]))
        copies[n].start()
    first = pl.multiple_of((y0 * blocks + x) * lines, lines)
    own_ref[...] = residual[pl.ds(first, lines), :]
    for copy in copies:
        copy.wait()


def group_rows(here, mixed, near_w, far_w, near_s, far_s, gain):
    lines, width = near_s.shape[1:]
    count = 8 * lines
    return pl.pallas_call(
        rows_kernel,
        out_shape=(
            jax.ShapeDtypeStruct((count, width), BF16),
            jax.ShapeDtypeStruct((lines, width), F32),
        ),
        in_specs=[pl.BlockSpec(memory_space=pltpu.SMEM)] + vmem(6),
        out_specs=[pl.BlockSpec(memory_space=pltpu.HBM)] + vmem(1),
        scratch_shapes=[
            pltpu.VMEM((count, width), F32),
            pltpu.VMEM((count, width), BF16),
            pltpu.SemaphoreType.DMA((4,)),
        ],
        cost_estimate=kernel_cost(2 * count * width * 1024, 2**23),
        compiler_params=pltpu.CompilerParams(vmem_limit_bytes=20 * 2**20),
        name="group_rows",
    )(here, mixed, near_w, far_w, near_s, far_s, gain)


CHUNKS = (2, 1, 1)
AHEAD = 2


def ffn_kernel(rows_ref, weight_ref, out_ref, rows, held, rows_sem, sems):
    z, _, _, kinds, lines, hidden_width = weight_ref.shape

    def copies(kind, n):
        each = z // CHUNKS[kind]
        span = pl.ds(n * each, each)
        return [
            pltpu.make_async_copy(
                weight_ref.at[span, y0, y1, kind],
                held.at[kind, span, y1, y0],
                sems.at[kind, n, 2 * y1 + y0],
            )
            for y1 in range(2)
            for y0 in range(2)
        ]

    order = [(kind, n) for kind in range(kinds) for n in range(CHUNKS[kind])]

    def start(at):
        for place in order[at : at + 1]:
            for copy in copies(*place):
                copy.start()

    def arrived(kind, n):
        each = z // CHUNKS[kind]
        for copy in copies(kind, n):
            copy.wait()
        start(order.index((kind, n)) + AHEAD)
        depth = each * 4 * lines
        return held[kind, n * each : (n + 1) * each].reshape(depth, hidden_width), depth

    fetch = pltpu.make_async_copy(rows_ref, rows, rows_sem)
    fetch.start()
    for at in range(AHEAD):
        start(at)
    fetch.wait()
    sums = []
    for kind in (0, 1):
        total = None
        for n in range(CHUNKS[kind]):
            block, depth = arrived(kind, n)
            part = dot(rows[:, n * depth : (n + 1) * depth], block)
            total = part if total is None else total + part
        sums.append(total)
    gate_sum, up_sum = sums
    hidden = (gate_sum * jax.nn.sigmoid(gate_sum) * up_sum).astype(BF16)
    for n in range(CHUNKS[2]):
        block, depth = arrived(2, n)
        out_ref[:, n * depth : (n + 1) * depth] = dot_nt(hidden, block).astype(BF16)


def feed_forward(rows, weights):
    count, width = rows.shape
    z, y0, y1, kinds, lines, hidden_width = weights.shape
    return pl.pallas_call(
        ffn_kernel,
        out_shape=jax.ShapeDtypeStruct((count, width), BF16),
        in_specs=[pl.BlockSpec(memory_space=pltpu.HBM)] * 2,
        out_specs=pl.BlockSpec(memory_space=pltpu.VMEM),
        scratch_shapes=[
            pltpu.VMEM((count, width), BF16),
            pltpu.VMEM((kinds, z, y1, y0, lines, hidden_width), BF16),
            pltpu.SemaphoreType.DMA,
            pltpu.SemaphoreType.DMA((kinds, max(CHUNKS), 4)),
        ],
        cost_estimate=kernel_cost(6 * count * width * hidden_width, 2**23, count * hidden_width),
        compiler_params=pltpu.CompilerParams(vmem_limit_bytes=52 * 2**20),
        name="feed_forward",
    )(rows, weights)


def moved(value, axes, place):
    lengths = [SIZES[a] for a in axes]
    pairs = []
    for y1 in range(lengths[0]):
        for y0 in range(lengths[1]):
            for c in range(lengths[2]):
                a, b, d = place(y1, y0, c)
                pairs.append(((y1 * 2 + y0) * 2 + c, (a * 2 + b) * 2 + d))
    return lax.ppermute(value, axes, pairs)


def shifted(value, axis, by):
    length = SIZES[axis]
    return lax.ppermute(value, axis, [(i, (i + by) % length) for i in range(length)])


def exchange(tiles, axes):
    return lax.all_to_all(tiles, axes, split_axis=0, concat_axis=0, tiled=True)


def gathered_weights(gate_weight, up_weight, down_weight):
    mine = jnp.concatenate([gate_weight, up_weight, down_weight.T], axis=0)
    lines, width = mine.shape
    axes = ("y1", "y0", "c")
    near = moved(mine, axes, lambda y1, y0, c: (y1, c, y0))
    far = moved(mine, axes, lambda y1, y0, c: (1 - y1, c, y0))
    upper = lax.axis_index("y1") == 1
    pair = jnp.stack([jnp.where(upper, far, near), jnp.where(upper, near, far)])
    whole = lax.all_gather(pair, Z + ("c",), axis=0)
    return whole.reshape(16, 2, 2, 3, lines // 3, width)


def layer(
    stream,
    queries,
    keys_in,
    values_in,
    gate_in,
    log_decay,
    head_gain,
    out_weight,
    norm_gain,
    gate_weight,
    up_weight,
    down_weight,
):
    weights = gathered_weights(gate_weight, up_weight, down_weight)
    rows, width = queries.shape[0], stream.shape[1]
    head_dim = queries.shape[1]
    sides = [shifted(out_weight, "x", 1), shifted(out_weight, "x", 3)]
    across = shifted(out_weight, "x", 2)
    others = [shifted(stream, "x", r) for r in (1, 2, 3)]
    near_w = jnp.concatenate([out_weight, sides[0], across, sides[1]], axis=0)
    near_s = jnp.stack([stream, *others])
    far_w = shifted(near_w, "c", 1)
    far_s = shifted(near_s, "y0", 1)
    within, carry_q, state = retention(
        queries, keys_in, values_in, log_decay.reshape(1, rows)
    )
    states = exchange(state, NEAR)
    joined = joined_state(states)
    joined = exchange(joined, "zh")
    zh = lax.axis_index("zh").astype(jnp.int32).reshape(1)
    entering = incoming_state(zh, joined, states)
    entering = exchange(entering, NEAR)
    entering = entering.reshape(head_dim, head_dim)
    sent = mix(within, carry_q, entering, gate_in, head_gain.reshape(1, -1))
    mixed = exchange(sent.reshape(16, *sent.shape[2:]), GROUP + ("c",))
    here = jnp.stack([lax.axis_index(a).astype(jnp.int32) for a in ("x", "c", "y0")])
    normed, residual = group_rows(
        here, mixed.reshape(2, 8, *mixed.shape[1:]), near_w, far_w, near_s, far_s, norm_gain.reshape(1, -1)
    )
    down_terms = feed_forward(normed, weights)
    mixer_out = exchange(down_terms.reshape(8, rows // 8, width), GROUP).astype(F32).sum(axis=0)
    return (residual + mixer_out).astype(BF16)


def solution(mesh):
    finer = Mesh(mesh.devices.reshape(*SIZES.values()), tuple(SIZES))
    return jax.shard_map(
        layer,
        mesh=finer,
        in_specs=(
            P(SP + TP, None),
            P(SP, TP),
            P(SP, TP),
            P(SP, TP),
            P(SP, TP),
            P(SP, TP),
            P(TP),
            P(TP, None),
            P(),
            P(SP, TP),
            P(SP, TP),
            P(TP, SP),
        ),
        out_specs=P(SP + TP, None),
        check_vma=False,
    )
```

```python
import jax
import jax.numpy as jnp
from jax import lax
from jax.experimental import pallas as pl
from jax.experimental.pallas import tpu as pltpu
from jax.sharding import Mesh
from jax.sharding import PartitionSpec as P


Z, Y = ("zh", "zl"), ("y1", "y0")
NEAR = ("zl",) + Y
SP = Z + Y
TP = ("x", "c")
GROUP = ("y0", "x")
SIZES = {"zh": 8, "zl": 2, "y1": 2, "y0": 2, "x": 4, "c": 2}
EPS = 1e-6
NEIGHBOURS = 8
F32, BF16 = jnp.float32, jnp.bfloat16


def vmem(count):
    return [pl.BlockSpec(memory_space=pltpu.VMEM)] * count


def kernel_cost(flops, moved, exps=0):
    return pl.CostEstimate(flops=flops, bytes_accessed=moved, transcendentals=exps)


def dot(a, b):
    return jnp.dot(a, b, preferred_element_type=F32)


def dot_nt(a, b):
    return lax.dot_general(a, b, (((1,), (1,)), ((), ())), preferred_element_type=F32)


def dot_tn(a, b):
    return lax.dot_general(a, b, (((0,), (0,)), ((), ())), preferred_element_type=F32)


def retention_kernel(q_ref, k_ref, v_ref, decay_ref, within_ref, carry_q_ref, state_ref):
    rows, head_dim = q_ref.shape
    scale = head_dim**-0.5
    at = lax.broadcasted_iota(jnp.int32, (rows, rows), 0)
    to = lax.broadcasted_iota(jnp.int32, (rows, rows), 1)
    causal = at >= to
    running = jnp.sum(jnp.where(causal, decay_ref[...], 0.0), axis=1, keepdims=True)
    across = jnp.sum(jnp.where(at == to, running, 0.0), axis=0, keepdims=True)
    total = running[rows - 1 : rows, :]
    q, k, v = q_ref[...], k_ref[...], v_ref[...]
    table = jnp.where(causal, jnp.exp(jnp.minimum(running - across, 0.0)), 0.0)
    scores = dot_nt(q, k) * scale
    within_ref[...] = dot((scores * table).astype(BF16), v)
    carry_q_ref[...] = (q.astype(F32) * jnp.exp(running)).astype(BF16)
    key_wide = (k.astype(F32) * scale * jnp.exp(total - running)).astype(BF16)
    state = dot_tn(key_wide, v)
    fill = jnp.broadcast_to(total, (8, head_dim))
    slices = state_ref.shape[0]
    part = head_dim // slices
    for n in range(slices):
        state_ref[n, :part, :] = state[n * part : (n + 1) * part]
        state_ref[n, part:, :] = fill


def retention(q, k, v, decay):
    rows, head_dim = q.shape
    part = head_dim // NEIGHBOURS
    return pl.pallas_call(
        retention_kernel,
        out_shape=(
            jax.ShapeDtypeStruct((rows, head_dim), F32),
            jax.ShapeDtypeStruct((rows, head_dim), BF16),
            jax.ShapeDtypeStruct((NEIGHBOURS, part + 8, head_dim), F32),
        ),
        in_specs=vmem(4),
        out_specs=vmem(3),
        cost_estimate=kernel_cost(6 * rows * rows * head_dim, 2**20, rows * rows),
        name="retention",
    )(q, k, v, decay)


def joined_kernel(states_ref, out_ref):
    part = states_ref.shape[1] - 8
    state = states_ref[0, :part, :]
    total = states_ref[0, part:, :]
    for n in range(1, states_ref.shape[0]):
        own = states_ref[n, part:, :]
        state = jnp.exp(own[:1]) * state + states_ref[n, :part, :]
        total = total + own
    high = total.astype(BF16).astype(F32)
    mid = (total - high).astype(BF16).astype(F32)
    line = lax.broadcasted_iota(jnp.int32, total.shape, 0)
    terms = jnp.where(line == 0, high, jnp.where(line == 1, mid, total - high - mid))
    packed = jnp.concatenate([state, terms], axis=0).astype(BF16)
    for n in range(out_ref.shape[0]):
        out_ref[n] = packed


def joined_state(states):
    _, lines, width = states.shape
    return pl.pallas_call(
        joined_kernel,
        out_shape=jax.ShapeDtypeStruct((SIZES["zh"], lines, width), BF16),
        in_specs=vmem(1),
        out_specs=pl.BlockSpec(memory_space=pltpu.VMEM),
        cost_estimate=kernel_cost(2**18, 2**18, 2**10),
        compiler_params=pltpu.CompilerParams(vmem_limit_bytes=2 * 2**20),
        name="joined_state",
    )(states)


def incoming_kernel(here_ref, joined_ref, states_ref, out_ref):
    part = out_ref.shape[1]
    here = here_ref[0]
    carried = jnp.zeros(out_ref.shape[1:], F32)
    for n in range(joined_ref.shape[0]):
        other = joined_ref[n].astype(F32)
        total = other[part : part + 1] + other[part + 1 : part + 2] + other[part + 2 : part + 3]
        after = jnp.exp(total) * carried + other[:part]
        carried = jnp.where(n < here, after, carried)
    for n in range(out_ref.shape[0]):
        out_ref[n] = carried
        carried = jnp.exp(states_ref[n, part : part + 1, :]) * carried + states_ref[n, :part, :]


def incoming_state(here, joined, states):
    count, lines, width = states.shape
    return pl.pallas_call(
        incoming_kernel,
        out_shape=jax.ShapeDtypeStruct((count, lines - 8, width), F32),
        in_specs=[pl.BlockSpec(memory_space=pltpu.SMEM)] + vmem(2),
        out_specs=pl.BlockSpec(memory_space=pltpu.VMEM),
        cost_estimate=kernel_cost(2**19, 2**19, 2**12),
        compiler_params=pltpu.CompilerParams(vmem_limit_bytes=2 * 2**20),
        name="incoming_state",
    )(here, joined, states)


def mix_kernel(within_ref, carry_q_ref, state_ref, gate_ref, gain_ref, out_ref):
    retained = within_ref[...] + dot(carry_q_ref[...], state_ref[...].astype(BF16))
    center = jnp.mean(retained, axis=-1, keepdims=True)
    off = retained - center
    spread = jnp.mean(off * off, axis=-1, keepdims=True)
    normed = off * lax.rsqrt(spread + EPS) * gain_ref[...].astype(F32)
    gate = gate_ref[...].astype(F32)
    mixed = (gate * jax.nn.sigmoid(gate) * normed).astype(BF16)
    places, cores, blocks, lines, _ = out_ref.shape
    for core in range(cores):
        for n in range(blocks):
            first = (n * cores + core) * lines
            piece = mixed[first : first + lines]
            for place in range(places):
                out_ref[place, core, n] = piece


def mix(within, carry_q, state, gate, gain):
    rows, width = within.shape
    return pl.pallas_call(
        mix_kernel,
        out_shape=jax.ShapeDtypeStruct((8, 2, 4, rows // 8, width), BF16),
        in_specs=vmem(5),
        out_specs=pl.BlockSpec(memory_space=pltpu.VMEM),
        cost_estimate=kernel_cost(2 * rows * width * width, 2**20, rows * width),
        name="mix",
    )(within, carry_q, state, gate, gain)


def rows_kernel(
    here_ref, mixed_ref, near_w_ref, far_w_ref, near_s_ref, far_s_ref, gain_ref, normed_ref, own_ref, residual, normed, sems
):
    halves, _, blocks, lines, head_dim = mixed_ref.shape
    count, width = normed_ref.shape
    x, c, y0 = here_ref[0], here_ref[1], here_ref[2]

    def heads_of(core):
        return jnp.concatenate(
            [
                jnp.concatenate(
                    [mixed_ref[n, ((x + 4 - r) % 4) * 2 + core].reshape(count // halves, head_dim) for r in range(4)],
                    axis=1,
                )
                for n in range(halves)
            ],
            axis=0,
        )

    near, far = heads_of(c), heads_of(1 - c)
    step = width // 4
    squares = jnp.zeros((count, 1), F32)
    for n in range(4):
        span = slice(n * step, (n + 1) * step)
        rows = []
        for half in range(halves):
            for block in range(blocks):
                at = (x + 4 - block) % 4
                rows.append(jnp.where(y0 == half, near_s_ref[at, :, span], far_s_ref[at, :, span]))
        part = (
            jnp.concatenate(rows, axis=0).astype(F32)
            + dot(near, near_w_ref[:, span])
            + dot(far, far_w_ref[:, span])
        )
        residual[:, span] = part
        squares += jnp.sum(part * part, axis=-1, keepdims=True)
    factor = lax.rsqrt(squares / width + EPS)
    copies = []
    for n in range(4):
        span = slice(n * step, (n + 1) * step)
        normed[:, span] = (residual[:, span] * factor * gain_ref[:, span].astype(F32)).astype(BF16)
        copies.append(pltpu.make_async_copy(normed.at[:, span], normed_ref.at[:, span], sems.at[n]))
        copies[n].start()
    first = pl.multiple_of((y0 * blocks + x) * lines, lines)
    own_ref[...] = residual[pl.ds(first, lines), :]
    for copy in copies:
        copy.wait()


def group_rows(here, mixed, near_w, far_w, near_s, far_s, gain):
    lines, width = near_s.shape[1:]
    count = 8 * lines
    return pl.pallas_call(
        rows_kernel,
        out_shape=(
            jax.ShapeDtypeStruct((count, width), BF16),
            jax.ShapeDtypeStruct((lines, width), F32),
        ),
        in_specs=[pl.BlockSpec(memory_space=pltpu.SMEM)] + vmem(6),
        out_specs=[pl.BlockSpec(memory_space=pltpu.HBM)] + vmem(1),
        scratch_shapes=[
            pltpu.VMEM((count, width), F32),
            pltpu.VMEM((count, width), BF16),
            pltpu.SemaphoreType.DMA((4,)),
        ],
        cost_estimate=kernel_cost(2 * count * width * 1024, 2**23),
        compiler_params=pltpu.CompilerParams(vmem_limit_bytes=20 * 2**20),
        name="group_rows",
    )(here, mixed, near_w, far_w, near_s, far_s, gain)


CHUNKS = (2, 1, 1)
AHEAD = 2


def ffn_kernel(rows_ref, weight_ref, out_ref, rows, held, rows_sem, sems):
    z, _, _, kinds, lines, hidden_width = weight_ref.shape

    def copies(kind, n):
        each = z // CHUNKS[kind]
        span = pl.ds(n * each, each)
        return [
            pltpu.make_async_copy(
                weight_ref.at[span, y0, y1, kind],
                held.at[kind, span, y1, y0],
                sems.at[kind, n, 2 * y1 + y0],
            )
            for y1 in range(2)
            for y0 in range(2)
        ]

    order = [(kind, n) for kind in range(kinds) for n in range(CHUNKS[kind])]

    def start(at):
        for place in order[at : at + 1]:
            for copy in copies(*place):
                copy.start()

    def arrived(kind, n):
        each = z // CHUNKS[kind]
        for copy in copies(kind, n):
            copy.wait()
        start(order.index((kind, n)) + AHEAD)
        depth = each * 4 * lines
        return held[kind, n * each : (n + 1) * each].reshape(depth, hidden_width), depth

    fetch = pltpu.make_async_copy(rows_ref, rows, rows_sem)
    fetch.start()
    for at in range(AHEAD):
        start(at)
    fetch.wait()
    sums = []
    for kind in (0, 1):
        total = None
        for n in range(CHUNKS[kind]):
            block, depth = arrived(kind, n)
            part = dot(rows[:, n * depth : (n + 1) * depth], block)
            total = part if total is None else total + part
        sums.append(total)
    gate_sum, up_sum = sums
    hidden = (gate_sum * jax.nn.sigmoid(gate_sum) * up_sum).astype(BF16)
    for n in range(CHUNKS[2]):
        block, depth = arrived(2, n)
        out_ref[:, n * depth : (n + 1) * depth] = dot_nt(hidden, block).astype(BF16)


def feed_forward(rows, weights):
    count, width = rows.shape
    z, y0, y1, kinds, lines, hidden_width = weights.shape
    return pl.pallas_call(
        ffn_kernel,
        out_shape=jax.ShapeDtypeStruct((count, width), BF16),
        in_specs=[pl.BlockSpec(memory_space=pltpu.HBM)] * 2,
        out_specs=pl.BlockSpec(memory_space=pltpu.VMEM),
        scratch_shapes=[
            pltpu.VMEM((count, width), BF16),
            pltpu.VMEM((kinds, z, y1, y0, lines, hidden_width), BF16),
            pltpu.SemaphoreType.DMA,
            pltpu.SemaphoreType.DMA((kinds, max(CHUNKS), 4)),
        ],
        cost_estimate=kernel_cost(6 * count * width * hidden_width, 2**23, count * hidden_width),
        compiler_params=pltpu.CompilerParams(vmem_limit_bytes=52 * 2**20),
        name="feed_forward",
    )(rows, weights)


def moved(value, axes, place):
    lengths = [SIZES[a] for a in axes]
    pairs = []
    for y1 in range(lengths[0]):
        for y0 in range(lengths[1]):
            for c in range(lengths[2]):
                a, b, d = place(y1, y0, c)
                pairs.append(((y1 * 2 + y0) * 2 + c, (a * 2 + b) * 2 + d))
    return lax.ppermute(value, axes, pairs)


def shifted(value, axis, by):
    length = SIZES[axis]
    return lax.ppermute(value, axis, [(i, (i + by) % length) for i in range(length)])


def exchange(tiles, axes):
    return lax.all_to_all(tiles, axes, split_axis=0, concat_axis=0, tiled=True)


def gathered_weights(gate_weight, up_weight, down_weight):
    mine = jnp.concatenate([gate_weight, up_weight, down_weight.T], axis=0)
    lines, width = mine.shape
    axes = ("y1", "y0", "c")
    near = moved(mine, axes, lambda y1, y0, c: (y1, c, y0))
    far = moved(mine, axes, lambda y1, y0, c: (1 - y1, c, y0))
    upper = lax.axis_index("y1") == 1
    pair = jnp.stack([jnp.where(upper, far, near), jnp.where(upper, near, far)])
    whole = lax.all_gather(pair, Z + ("c",), axis=0)
    return whole.reshape(16, 2, 2, 3, lines // 3, width)


def layer(
    stream,
    queries,
    keys_in,
    values_in,
    gate_in,
    log_decay,
    head_gain,
    out_weight,
    norm_gain,
    gate_weight,
    up_weight,
    down_weight,
):
    weights = gathered_weights(gate_weight, up_weight, down_weight)
    rows, width = queries.shape[0], stream.shape[1]
    head_dim = queries.shape[1]
    found = [out_weight] + [shifted(out_weight, "x", r) for r in (1, 2, 3)]
    others = [shifted(stream, "x", r) for r in (1, 2, 3)]
    near_s = jnp.stack([stream, *others])
    far_s = shifted(near_s, "y0", 1)
    near_w = jnp.concatenate(found, axis=0)
    far_w = shifted(near_w, "c", 1)
    within, carry_q, state = retention(
        queries, keys_in, values_in, log_decay.reshape(1, rows)
    )
    states = exchange(state, NEAR)
    joined = joined_state(states)
    joined = exchange(joined, "zh")
    zh = lax.axis_index("zh").astype(jnp.int32).reshape(1)
    entering = incoming_state(zh, joined, states)
    entering = exchange(entering, NEAR)
    entering = entering.reshape(head_dim, head_dim)
    sent = mix(within, carry_q, entering, gate_in, head_gain.reshape(1, -1))
    mixed = exchange(sent.reshape(16, *sent.shape[2:]), GROUP + ("c",))
    here = jnp.stack([lax.axis_index(a).astype(jnp.int32) for a in ("x", "c", "y0")])
    normed, residual = group_rows(
        here, mixed.reshape(2, 8, *mixed.shape[1:]), near_w, far_w, near_s, far_s, norm_gain.reshape(1, -1)
    )
    down_terms = feed_forward(normed, weights)
    mixer_out = exchange(down_terms.reshape(8, rows // 8, width), GROUP).astype(F32).sum(axis=0)
    return (residual + mixer_out).astype(BF16)


def solution(mesh):
    finer = Mesh(mesh.devices.reshape(*SIZES.values()), tuple(SIZES))
    return jax.shard_map(
        layer,
        mesh=finer,
        in_specs=(
            P(SP + TP, None),
            P(SP, TP),
            P(SP, TP),
            P(SP, TP),
            P(SP, TP),
            P(SP, TP),
            P(TP),
            P(TP, None),
            P(),
            P(SP, TP),
            P(SP, TP),
            P(TP, SP),
        ),
        out_specs=P(SP + TP, None),
        check_vma=False,
    )
```

```python
import jax
import jax.numpy as jnp
from jax import lax
from jax.experimental import pallas as pl
from jax.experimental.pallas import tpu as pltpu
from jax.sharding import Mesh
from jax.sharding import PartitionSpec as P


Z, Y = ("zh", "zl"), ("y1", "y0")
NEAR = ("zl",) + Y
SP = Z + Y
TP = ("x", "c")
GROUP = ("y0", "x")
SIZES = {"zh": 8, "zl": 2, "y1": 2, "y0": 2, "x": 4, "c": 2}
EPS = 1e-6
NEIGHBOURS = 8
F32, BF16 = jnp.float32, jnp.bfloat16


def vmem(count):
    return [pl.BlockSpec(memory_space=pltpu.VMEM)] * count


def kernel_cost(flops, moved, exps=0):
    return pl.CostEstimate(flops=flops, bytes_accessed=moved, transcendentals=exps)


def dot(a, b):
    return jnp.dot(a, b, preferred_element_type=F32)


def dot_nt(a, b):
    return lax.dot_general(a, b, (((1,), (1,)), ((), ())), preferred_element_type=F32)


def dot_tn(a, b):
    return lax.dot_general(a, b, (((0,), (0,)), ((), ())), preferred_element_type=F32)


def retention_kernel(q_ref, k_ref, v_ref, decay_ref, within_ref, carry_q_ref, state_ref):
    rows, head_dim = q_ref.shape
    scale = head_dim**-0.5
    at = lax.broadcasted_iota(jnp.int32, (rows, rows), 0)
    to = lax.broadcasted_iota(jnp.int32, (rows, rows), 1)
    causal = at >= to
    running = jnp.sum(jnp.where(causal, decay_ref[...], 0.0), axis=1, keepdims=True)
    across = jnp.sum(jnp.where(at == to, running, 0.0), axis=0, keepdims=True)
    total = running[rows - 1 : rows, :]
    q, k, v = q_ref[...], k_ref[...], v_ref[...]
    table = jnp.where(causal, jnp.exp(jnp.minimum(running - across, 0.0)), 0.0)
    scores = dot_nt(q, k) * scale
    within_ref[...] = dot((scores * table).astype(BF16), v)
    carry_q_ref[...] = (q.astype(F32) * jnp.exp(running)).astype(BF16)
    key_wide = (k.astype(F32) * scale * jnp.exp(total - running)).astype(BF16)
    state = dot_tn(key_wide, v)
    fill = jnp.broadcast_to(total, (8, head_dim))
    slices = state_ref.shape[0]
    part = head_dim // slices
    for n in range(slices):
        state_ref[n, :part, :] = state[n * part : (n + 1) * part]
        state_ref[n, part:, :] = fill


def retention(q, k, v, decay):
    rows, head_dim = q.shape
    part = head_dim // NEIGHBOURS
    return pl.pallas_call(
        retention_kernel,
        out_shape=(
            jax.ShapeDtypeStruct((rows, head_dim), F32),
            jax.ShapeDtypeStruct((rows, head_dim), BF16),
            jax.ShapeDtypeStruct((NEIGHBOURS, part + 8, head_dim), F32),
        ),
        in_specs=vmem(4),
        out_specs=vmem(3),
        cost_estimate=kernel_cost(6 * rows * rows * head_dim, 2**20, rows * rows),
        name="retention",
    )(q, k, v, decay)


def joined_kernel(states_ref, out_ref):
    part = states_ref.shape[1] - 8
    state = states_ref[0, :part, :]
    total = states_ref[0, part:, :]
    for n in range(1, states_ref.shape[0]):
        own = states_ref[n, part:, :]
        state = jnp.exp(own[:1]) * state + states_ref[n, :part, :]
        total = total + own
    high = total.astype(BF16).astype(F32)
    mid = (total - high).astype(BF16).astype(F32)
    line = lax.broadcasted_iota(jnp.int32, total.shape, 0)
    terms = jnp.where(line == 0, high, jnp.where(line == 1, mid, total - high - mid))
    packed = jnp.concatenate([state, terms], axis=0).astype(BF16)
    for n in range(out_ref.shape[0]):
        out_ref[n] = packed


def joined_state(states):
    _, lines, width = states.shape
    return pl.pallas_call(
        joined_kernel,
        out_shape=jax.ShapeDtypeStruct((SIZES["zh"], lines, width), BF16),
        in_specs=vmem(1),
        out_specs=pl.BlockSpec(memory_space=pltpu.VMEM),
        cost_estimate=kernel_cost(2**18, 2**18, 2**10),
        compiler_params=pltpu.CompilerParams(vmem_limit_bytes=2 * 2**20),
        name="joined_state",
    )(states)


def incoming_kernel(here_ref, joined_ref, states_ref, out_ref):
    part = out_ref.shape[1]
    here = here_ref[0]
    carried = jnp.zeros(out_ref.shape[1:], F32)
    for n in range(joined_ref.shape[0]):
        other = joined_ref[n].astype(F32)
        total = other[part : part + 1] + other[part + 1 : part + 2] + other[part + 2 : part + 3]
        after = jnp.exp(total) * carried + other[:part]
        carried = jnp.where(n < here, after, carried)
    for n in range(out_ref.shape[0]):
        out_ref[n] = carried
        carried = jnp.exp(states_ref[n, part : part + 1, :]) * carried + states_ref[n, :part, :]


def incoming_state(here, joined, states):
    count, lines, width = states.shape
    return pl.pallas_call(
        incoming_kernel,
        out_shape=jax.ShapeDtypeStruct((count, lines - 8, width), F32),
        in_specs=[pl.BlockSpec(memory_space=pltpu.SMEM)] + vmem(2),
        out_specs=pl.BlockSpec(memory_space=pltpu.VMEM),
        cost_estimate=kernel_cost(2**19, 2**19, 2**12),
        compiler_params=pltpu.CompilerParams(vmem_limit_bytes=2 * 2**20),
        name="incoming_state",
    )(here, joined, states)


def mix_kernel(within_ref, carry_q_ref, state_ref, gate_ref, gain_ref, out_ref):
    retained = within_ref[...] + dot(carry_q_ref[...], state_ref[...].astype(BF16))
    center = jnp.mean(retained, axis=-1, keepdims=True)
    off = retained - center
    spread = jnp.mean(off * off, axis=-1, keepdims=True)
    normed = off * lax.rsqrt(spread + EPS) * gain_ref[...].astype(F32)
    gate = gate_ref[...].astype(F32)
    mixed = (gate * jax.nn.sigmoid(gate) * normed).astype(BF16)
    places, cores, blocks, lines, _ = out_ref.shape
    for core in range(cores):
        for n in range(blocks):
            first = (n * cores + core) * lines
            piece = mixed[first : first + lines]
            for place in range(places):
                out_ref[place, core, n] = piece


def mix(within, carry_q, state, gate, gain):
    rows, width = within.shape
    return pl.pallas_call(
        mix_kernel,
        out_shape=jax.ShapeDtypeStruct((8, 2, 4, rows // 8, width), BF16),
        in_specs=vmem(5),
        out_specs=pl.BlockSpec(memory_space=pltpu.VMEM),
        cost_estimate=kernel_cost(2 * rows * width * width, 2**20, rows * width),
        name="mix",
    )(within, carry_q, state, gate, gain)


def rows_kernel(
    here_ref, mixed_ref, near_w_ref, far_w_ref, near_s_ref, far_s_ref, gain_ref, normed_ref, own_ref, residual, normed, sems
):
    halves, _, blocks, lines, head_dim = mixed_ref.shape
    count, width = normed_ref.shape
    x, c, y0 = here_ref[0], here_ref[1], here_ref[2]

    def heads_of(core):
        return jnp.concatenate(
            [
                jnp.concatenate(
                    [mixed_ref[n, ((x + 4 - r) % 4) * 2 + core].reshape(count // halves, head_dim) for r in range(4)],
                    axis=1,
                )
                for n in range(halves)
            ],
            axis=0,
        )

    near, far = heads_of(c), heads_of(1 - c)
    step = width // 4
    squares = jnp.zeros((count, 1), F32)
    for n in range(4):
        span = slice(n * step, (n + 1) * step)
        rows = []
        for half in range(halves):
            for block in range(blocks):
                at = (x + 4 - block) % 4
                rows.append(jnp.where(y0 == half, near_s_ref[at, :, span], far_s_ref[at, :, span]))
        part = (
            jnp.concatenate(rows, axis=0).astype(F32)
            + dot(near, near_w_ref[:, span])
            + dot(far, far_w_ref[:, span])
        )
        residual[:, span] = part
        squares += jnp.sum(part * part, axis=-1, keepdims=True)
    factor = lax.rsqrt(squares / width + EPS)
    copies = []
    for n in range(4):
        span = slice(n * step, (n + 1) * step)
        normed[:, span] = (residual[:, span] * factor * gain_ref[:, span].astype(F32)).astype(BF16)
        copies.append(pltpu.make_async_copy(normed.at[:, span], normed_ref.at[:, span], sems.at[n]))
        copies[n].start()
    first = pl.multiple_of((y0 * blocks + x) * lines, lines)
    own_ref[...] = residual[pl.ds(first, lines), :]
    for copy in copies:
        copy.wait()


def group_rows(here, mixed, near_w, far_w, near_s, far_s, gain):
    lines, width = near_s.shape[1:]
    count = 8 * lines
    return pl.pallas_call(
        rows_kernel,
        out_shape=(
            jax.ShapeDtypeStruct((count, width), BF16),
            jax.ShapeDtypeStruct((lines, width), F32),
        ),
        in_specs=[pl.BlockSpec(memory_space=pltpu.SMEM)] + vmem(6),
        out_specs=[pl.BlockSpec(memory_space=pltpu.HBM)] + vmem(1),
        scratch_shapes=[
            pltpu.VMEM((count, width), F32),
            pltpu.VMEM((count, width), BF16),
            pltpu.SemaphoreType.DMA((4,)),
        ],
        cost_estimate=kernel_cost(2 * count * width * 1024, 2**23),
        compiler_params=pltpu.CompilerParams(vmem_limit_bytes=20 * 2**20),
        name="group_rows",
    )(here, mixed, near_w, far_w, near_s, far_s, gain)


CHUNKS = (2, 1, 1)
AHEAD = 2


def ffn_kernel(rows_ref, weight_ref, out_ref, rows, held, rows_sem, sems):
    z, _, _, kinds, lines, hidden_width = weight_ref.shape

    def copies(kind, n):
        each = z // CHUNKS[kind]
        span = pl.ds(n * each, each)
        return [
            pltpu.make_async_copy(
                weight_ref.at[span, y0, y1, kind],
                held.at[kind, span, y1, y0],
                sems.at[kind, n, 2 * y1 + y0],
            )
            for y1 in range(2)
            for y0 in range(2)
        ]

    order = [(kind, n) for kind in range(kinds) for n in range(CHUNKS[kind])]

    def start(at):
        for place in order[at : at + 1]:
            for copy in copies(*place):
                copy.start()

    def arrived(kind, n):
        each = z // CHUNKS[kind]
        for copy in copies(kind, n):
            copy.wait()
        start(order.index((kind, n)) + AHEAD)
        depth = each * 4 * lines
        return held[kind, n * each : (n + 1) * each].reshape(depth, hidden_width), depth

    fetch = pltpu.make_async_copy(rows_ref, rows, rows_sem)
    start(0)
    fetch.start()
    for at in range(1, AHEAD):
        start(at)
    fetch.wait()
    sums = []
    for kind in (0, 1):
        total = None
        for n in range(CHUNKS[kind]):
            block, depth = arrived(kind, n)
            part = dot(rows[:, n * depth : (n + 1) * depth], block)
            total = part if total is None else total + part
        sums.append(total)
    gate_sum, up_sum = sums
    hidden = (gate_sum * jax.nn.sigmoid(gate_sum) * up_sum).astype(BF16)
    for n in range(CHUNKS[2]):
        block, depth = arrived(2, n)
        out_ref[:, n * depth : (n + 1) * depth] = dot_nt(hidden, block).astype(BF16)


def feed_forward(rows, weights):
    count, width = rows.shape
    z, y0, y1, kinds, lines, hidden_width = weights.shape
    return pl.pallas_call(
        ffn_kernel,
        out_shape=jax.ShapeDtypeStruct((count, width), BF16),
        in_specs=[pl.BlockSpec(memory_space=pltpu.HBM)] * 2,
        out_specs=pl.BlockSpec(memory_space=pltpu.VMEM),
        scratch_shapes=[
            pltpu.VMEM((count, width), BF16),
            pltpu.VMEM((kinds, z, y1, y0, lines, hidden_width), BF16),
            pltpu.SemaphoreType.DMA,
            pltpu.SemaphoreType.DMA((kinds, max(CHUNKS), 4)),
        ],
        cost_estimate=kernel_cost(6 * count * width * hidden_width, 2**23, count * hidden_width),
        compiler_params=pltpu.CompilerParams(vmem_limit_bytes=52 * 2**20),
        name="feed_forward",
    )(rows, weights)


def moved(value, axes, place):
    lengths = [SIZES[a] for a in axes]
    pairs = []
    for y1 in range(lengths[0]):
        for y0 in range(lengths[1]):
            for c in range(lengths[2]):
                a, b, d = place(y1, y0, c)
                pairs.append(((y1 * 2 + y0) * 2 + c, (a * 2 + b) * 2 + d))
    return lax.ppermute(value, axes, pairs)


def shifted(value, axis, by):
    length = SIZES[axis]
    return lax.ppermute(value, axis, [(i, (i + by) % length) for i in range(length)])


def exchange(tiles, axes):
    return lax.all_to_all(tiles, axes, split_axis=0, concat_axis=0, tiled=True)


def gathered_weights(gate_weight, up_weight, down_weight):
    mine = jnp.concatenate([gate_weight, up_weight, down_weight.T], axis=0)
    lines, width = mine.shape
    axes = ("y1", "y0", "c")
    near = moved(mine, axes, lambda y1, y0, c: (y1, c, y0))
    far = moved(mine, axes, lambda y1, y0, c: (1 - y1, c, y0))
    upper = lax.axis_index("y1") == 1
    pair = jnp.stack([jnp.where(upper, far, near), jnp.where(upper, near, far)])
    whole = lax.all_gather(pair, Z + ("c",), axis=0)
    return whole.reshape(16, 2, 2, 3, lines // 3, width)


def layer(
    stream,
    queries,
    keys_in,
    values_in,
    gate_in,
    log_decay,
    head_gain,
    out_weight,
    norm_gain,
    gate_weight,
    up_weight,
    down_weight,
):
    weights = gathered_weights(gate_weight, up_weight, down_weight)
    rows, width = queries.shape[0], stream.shape[1]
    head_dim = queries.shape[1]
    found = [out_weight] + [shifted(out_weight, "x", r) for r in (1, 2, 3)]
    others = [shifted(stream, "x", r) for r in (1, 2, 3)]
    near_s = jnp.stack([stream, *others])
    far_s = shifted(near_s, "y0", 1)
    near_w = jnp.concatenate(found, axis=0)
    far_w = shifted(near_w, "c", 1)
    within, carry_q, state = retention(
        queries, keys_in, values_in, log_decay.reshape(1, rows)
    )
    states = exchange(state, NEAR)
    joined = joined_state(states)
    joined = exchange(joined, "zh")
    zh = lax.axis_index("zh").astype(jnp.int32).reshape(1)
    entering = incoming_state(zh, joined, states)
    entering = exchange(entering, NEAR)
    entering = entering.reshape(head_dim, head_dim)
    sent = mix(within, carry_q, entering, gate_in, head_gain.reshape(1, -1))
    mixed = exchange(sent.reshape(16, *sent.shape[2:]), GROUP + ("c",))
    here = jnp.stack([lax.axis_index(a).astype(jnp.int32) for a in ("x", "c", "y0")])
    normed, residual = group_rows(
        here, mixed.reshape(2, 8, *mixed.shape[1:]), near_w, far_w, near_s, far_s, norm_gain.reshape(1, -1)
    )
    down_terms = feed_forward(normed, weights)
    terms = exchange(down_terms.reshape(8, rows // 8, width), GROUP)
    result = residual
    for n in range(8):
        result = result + terms[n].astype(F32)
    return result.astype(BF16)


def solution(mesh):
    finer = Mesh(mesh.devices.reshape(*SIZES.values()), tuple(SIZES))
    return jax.shard_map(
        layer,
        mesh=finer,
        in_specs=(
            P(SP + TP, None),
            P(SP, TP),
            P(SP, TP),
            P(SP, TP),
            P(SP, TP),
            P(SP, TP),
            P(TP),
            P(TP, None),
            P(),
            P(SP, TP),
            P(SP, TP),
            P(TP, SP),
        ),
        out_specs=P(SP + TP, None),
        check_vma=False,
    )
```

```python
import jax
import jax.numpy as jnp
from jax import lax
from jax.experimental import pallas as pl
from jax.experimental.pallas import tpu as pltpu
from jax.sharding import Mesh
from jax.sharding import PartitionSpec as P


Z, Y = ("zh", "zl"), ("y1", "y0")
NEAR = ("zl",) + Y
SP = Z + Y
TP = ("x", "c")
GROUP = ("y0", "x")
SIZES = {"zh": 8, "zl": 2, "y1": 2, "y0": 2, "x": 4, "c": 2}
EPS = 1e-6
NEIGHBOURS = 8
F32, BF16 = jnp.float32, jnp.bfloat16


def vmem(count):
    return [pl.BlockSpec(memory_space=pltpu.VMEM)] * count


def kernel_cost(flops, moved, exps=0):
    return pl.CostEstimate(flops=flops, bytes_accessed=moved, transcendentals=exps)


def dot(a, b):
    return jnp.dot(a, b, preferred_element_type=F32)


def dot_nt(a, b):
    return lax.dot_general(a, b, (((1,), (1,)), ((), ())), preferred_element_type=F32)


def dot_tn(a, b):
    return lax.dot_general(a, b, (((0,), (0,)), ((), ())), preferred_element_type=F32)


def retention_kernel(q_ref, k_ref, v_ref, decay_ref, within_ref, carry_q_ref, state_ref):
    rows, head_dim = q_ref.shape
    scale = head_dim**-0.5
    at = lax.broadcasted_iota(jnp.int32, (rows, rows), 0)
    to = lax.broadcasted_iota(jnp.int32, (rows, rows), 1)
    causal = at >= to
    running = jnp.sum(jnp.where(causal, decay_ref[...], 0.0), axis=1, keepdims=True)
    across = jnp.sum(jnp.where(at == to, running, 0.0), axis=0, keepdims=True)
    total = running[rows - 1 : rows, :]
    q, k, v = q_ref[...], k_ref[...], v_ref[...]
    table = jnp.where(causal, jnp.exp(jnp.minimum(running - across, 0.0)), 0.0)
    scores = dot_nt(q, k) * scale
    within_ref[...] = dot((scores * table).astype(BF16), v)
    carry_q_ref[...] = (q.astype(F32) * jnp.exp(running)).astype(BF16)
    key_wide = (k.astype(F32) * scale * jnp.exp(total - running)).astype(BF16)
    state = dot_tn(key_wide, v)
    fill = jnp.broadcast_to(total, (8, head_dim))
    slices = state_ref.shape[0]
    part = head_dim // slices
    for n in range(slices):
        state_ref[n, :part, :] = state[n * part : (n + 1) * part]
        state_ref[n, part:, :] = fill


def retention(q, k, v, decay):
    rows, head_dim = q.shape
    part = head_dim // NEIGHBOURS
    return pl.pallas_call(
        retention_kernel,
        out_shape=(
            jax.ShapeDtypeStruct((rows, head_dim), F32),
            jax.ShapeDtypeStruct((rows, head_dim), BF16),
            jax.ShapeDtypeStruct((NEIGHBOURS, part + 8, head_dim), F32),
        ),
        in_specs=vmem(4),
        out_specs=vmem(3),
        cost_estimate=kernel_cost(6 * rows * rows * head_dim, 2**20, rows * rows),
        name="retention",
    )(q, k, v, decay)


def joined_kernel(states_ref, out_ref):
    part = states_ref.shape[1] - 8
    state = states_ref[0, :part, :]
    total = states_ref[0, part:, :]
    for n in range(1, states_ref.shape[0]):
        own = states_ref[n, part:, :]
        state = jnp.exp(own[:1]) * state + states_ref[n, :part, :]
        total = total + own
    high = total.astype(BF16).astype(F32)
    mid = (total - high).astype(BF16).astype(F32)
    line = lax.broadcasted_iota(jnp.int32, total.shape, 0)
    terms = jnp.where(line == 0, high, jnp.where(line == 1, mid, total - high - mid))
    packed = jnp.concatenate([state, terms], axis=0).astype(BF16)
    for n in range(out_ref.shape[0]):
        out_ref[n] = packed


def joined_state(states):
    _, lines, width = states.shape
    return pl.pallas_call(
        joined_kernel,
        out_shape=jax.ShapeDtypeStruct((SIZES["zh"], lines, width), BF16),
        in_specs=vmem(1),
        out_specs=pl.BlockSpec(memory_space=pltpu.VMEM),
        cost_estimate=kernel_cost(2**18, 2**18, 2**10),
        compiler_params=pltpu.CompilerParams(vmem_limit_bytes=2 * 2**20),
        name="joined_state",
    )(states)


def incoming_kernel(here_ref, joined_ref, states_ref, out_ref):
    part = out_ref.shape[1]
    here = here_ref[0]
    carried = jnp.zeros(out_ref.shape[1:], F32)
    for n in range(joined_ref.shape[0]):
        other = joined_ref[n].astype(F32)
        total = other[part : part + 1] + other[part + 1 : part + 2] + other[part + 2 : part + 3]
        after = jnp.exp(total) * carried + other[:part]
        carried = jnp.where(n < here, after, carried)
    for n in range(out_ref.shape[0]):
        out_ref[n] = carried
        carried = jnp.exp(states_ref[n, part : part + 1, :]) * carried + states_ref[n, :part, :]


def incoming_state(here, joined, states):
    count, lines, width = states.shape
    return pl.pallas_call(
        incoming_kernel,
        out_shape=jax.ShapeDtypeStruct((count, lines - 8, width), F32),
        in_specs=[pl.BlockSpec(memory_space=pltpu.SMEM)] + vmem(2),
        out_specs=pl.BlockSpec(memory_space=pltpu.VMEM),
        cost_estimate=kernel_cost(2**19, 2**19, 2**12),
        compiler_params=pltpu.CompilerParams(vmem_limit_bytes=2 * 2**20),
        name="incoming_state",
    )(here, joined, states)


def mix_kernel(within_ref, carry_q_ref, state_ref, gate_ref, gain_ref, out_ref):
    retained = within_ref[...] + dot(carry_q_ref[...], state_ref[...].astype(BF16))
    center = jnp.mean(retained, axis=-1, keepdims=True)
    off = retained - center
    spread = jnp.mean(off * off, axis=-1, keepdims=True)
    normed = off * lax.rsqrt(spread + EPS) * gain_ref[...].astype(F32)
    gate = gate_ref[...].astype(F32)
    mixed = (gate * jax.nn.sigmoid(gate) * normed).astype(BF16)
    places, cores, blocks, lines, _ = out_ref.shape
    for core in range(cores):
        for n in range(blocks):
            first = (n * cores + core) * lines
            piece = mixed[first : first + lines]
            for place in range(places):
                out_ref[place, core, n] = piece


def mix(within, carry_q, state, gate, gain):
    rows, width = within.shape
    return pl.pallas_call(
        mix_kernel,
        out_shape=jax.ShapeDtypeStruct((8, 2, 4, rows // 8, width), BF16),
        in_specs=vmem(5),
        out_specs=pl.BlockSpec(memory_space=pltpu.VMEM),
        cost_estimate=kernel_cost(2 * rows * width * width, 2**20, rows * width),
        name="mix",
    )(within, carry_q, state, gate, gain)


def rows_kernel(
    here_ref, mixed_ref, near_w_ref, far_w_ref, near_s_ref, far_s_ref, gain_ref, normed_ref, own_ref, residual, normed, sems
):
    halves, _, blocks, lines, head_dim = mixed_ref.shape
    count, width = normed_ref.shape
    x, c, y0 = here_ref[0], here_ref[1], here_ref[2]

    def heads_of(core):
        return jnp.concatenate(
            [
                jnp.concatenate(
                    [mixed_ref[n, ((x + 4 - r) % 4) * 2 + core].reshape(count // halves, head_dim) for r in range(4)],
                    axis=1,
                )
                for n in range(halves)
            ],
            axis=0,
        )

    near, far = heads_of(c), heads_of(1 - c)
    step = width // 4
    squares = jnp.zeros((count, 1), F32)
    for n in range(4):
        span = slice(n * step, (n + 1) * step)
        rows = []
        for half in range(halves):
            for block in range(blocks):
                at = (x + 4 - block) % 4
                rows.append(jnp.where(y0 == half, near_s_ref[at, :, span], far_s_ref[at, :, span]))
        part = (
            jnp.concatenate(rows, axis=0).astype(F32)
            + dot(near, near_w_ref[:, span])
            + dot(far, far_w_ref[:, span])
        )
        residual[:, span] = part
        squares += jnp.sum(part * part, axis=-1, keepdims=True)
    factor = lax.rsqrt(squares / width + EPS)
    copies = []
    for n in range(4):
        span = slice(n * step, (n + 1) * step)
        normed[:, span] = (residual[:, span] * factor * gain_ref[:, span].astype(F32)).astype(BF16)
        copies.append(pltpu.make_async_copy(normed.at[:, span], normed_ref.at[:, span], sems.at[n]))
        copies[n].start()
    first = pl.multiple_of((y0 * blocks + x) * lines, lines)
    own_ref[...] = residual[pl.ds(first, lines), :]
    for copy in copies:
        copy.wait()


def group_rows(here, mixed, near_w, far_w, near_s, far_s, gain):
    lines, width = near_s.shape[1:]
    count = 8 * lines
    return pl.pallas_call(
        rows_kernel,
        out_shape=(
            jax.ShapeDtypeStruct((count, width), BF16),
            jax.ShapeDtypeStruct((lines, width), F32),
        ),
        in_specs=[pl.BlockSpec(memory_space=pltpu.SMEM)] + vmem(6),
        out_specs=[pl.BlockSpec(memory_space=pltpu.HBM)] + vmem(1),
        scratch_shapes=[
            pltpu.VMEM((count, width), F32),
            pltpu.VMEM((count, width), BF16),
            pltpu.SemaphoreType.DMA((4,)),
        ],
        cost_estimate=kernel_cost(2 * count * width * 1024, 2**23),
        compiler_params=pltpu.CompilerParams(vmem_limit_bytes=20 * 2**20),
        name="group_rows",
    )(here, mixed, near_w, far_w, near_s, far_s, gain)


CHUNKS = (2, 1, 1)
AHEAD = 2


def ffn_kernel(y1_ref, rows_ref, weight_ref, out_ref, rows, held, rows_sem, sems):
    z, _, _, kinds, lines, hidden_width = weight_ref.shape

    def copies(kind, n):
        each = z // CHUNKS[kind]
        span = pl.ds(n * each, each)
        return [
            pltpu.make_async_copy(
                weight_ref.at[span, y0, jnp.where(y1_ref[0] == y1, 0, 1), kind],
                held.at[kind, span, y1, y0],
                sems.at[kind, n, 2 * y1 + y0],
            )
            for y1 in range(2)
            for y0 in range(2)
        ]

    order = [(kind, n) for kind in range(kinds) for n in range(CHUNKS[kind])]

    def start(at):
        for place in order[at : at + 1]:
            for copy in copies(*place):
                copy.start()

    def arrived(kind, n):
        each = z // CHUNKS[kind]
        for copy in copies(kind, n):
            copy.wait()
        start(order.index((kind, n)) + AHEAD)
        depth = each * 4 * lines
        return held[kind, n * each : (n + 1) * each].reshape(depth, hidden_width), depth

    fetch = pltpu.make_async_copy(rows_ref, rows, rows_sem)
    start(0)
    fetch.start()
    for at in range(1, AHEAD):
        start(at)
    fetch.wait()
    sums = []
    for kind in (0, 1):
        total = None
        for n in range(CHUNKS[kind]):
            block, depth = arrived(kind, n)
            part = dot(rows[:, n * depth : (n + 1) * depth], block)
            total = part if total is None else total + part
        sums.append(total)
    gate_sum, up_sum = sums
    hidden = (gate_sum * jax.nn.sigmoid(gate_sum) * up_sum).astype(BF16)
    for n in range(CHUNKS[2]):
        block, depth = arrived(2, n)
        out_ref[:, n * depth : (n + 1) * depth] = dot_nt(hidden, block).astype(BF16)


def feed_forward(here, rows, weights):
    count, width = rows.shape
    z, y0, y1, kinds, lines, hidden_width = weights.shape
    return pl.pallas_call(
        ffn_kernel,
        out_shape=jax.ShapeDtypeStruct((count, width), BF16),
        in_specs=[pl.BlockSpec(memory_space=pltpu.SMEM)] + [pl.BlockSpec(memory_space=pltpu.HBM)] * 2,
        out_specs=pl.BlockSpec(memory_space=pltpu.VMEM),
        scratch_shapes=[
            pltpu.VMEM((count, width), BF16),
            pltpu.VMEM((kinds, z, y1, y0, lines, hidden_width), BF16),
            pltpu.SemaphoreType.DMA,
            pltpu.SemaphoreType.DMA((kinds, max(CHUNKS), 4)),
        ],
        cost_estimate=kernel_cost(6 * count * width * hidden_width, 2**23, count * hidden_width),
        compiler_params=pltpu.CompilerParams(vmem_limit_bytes=52 * 2**20),
        name="feed_forward",
    )(here, rows, weights)


def moved(value, axes, place):
    lengths = [SIZES[a] for a in axes]
    pairs = []
    for y1 in range(lengths[0]):
        for y0 in range(lengths[1]):
            for c in range(lengths[2]):
                a, b, d = place(y1, y0, c)
                pairs.append(((y1 * 2 + y0) * 2 + c, (a * 2 + b) * 2 + d))
    return lax.ppermute(value, axes, pairs)


def shifted(value, axis, by):
    length = SIZES[axis]
    return lax.ppermute(value, axis, [(i, (i + by) % length) for i in range(length)])


def exchange(tiles, axes):
    return lax.all_to_all(tiles, axes, split_axis=0, concat_axis=0, tiled=True)


def gathered_weights(gate_weight, up_weight, down_weight):
    mine = jnp.concatenate([gate_weight, up_weight, down_weight.T], axis=0)
    lines, width = mine.shape
    axes = ("y1", "y0", "c")
    near = moved(mine, axes, lambda y1, y0, c: (y1, c, y0))
    far = moved(mine, axes, lambda y1, y0, c: (1 - y1, c, y0))
    pair = jnp.concatenate([near, far], axis=0)
    whole = lax.all_gather(pair, Z + ("c",), axis=0)
    return whole.reshape(16, 2, 2, 3, lines // 3, width)


def layer(
    stream,
    queries,
    keys_in,
    values_in,
    gate_in,
    log_decay,
    head_gain,
    out_weight,
    norm_gain,
    gate_weight,
    up_weight,
    down_weight,
):
    weights = gathered_weights(gate_weight, up_weight, down_weight)
    rows, width = queries.shape[0], stream.shape[1]
    head_dim = queries.shape[1]
    found = [out_weight] + [shifted(out_weight, "x", r) for r in (1, 2, 3)]
    others = [shifted(stream, "x", r) for r in (1, 2, 3)]
    near_s = jnp.stack([stream, *others])
    far_s = shifted(near_s, "y0", 1)
    near_w = jnp.concatenate(found, axis=0)
    far_w = shifted(near_w, "c", 1)
    within, carry_q, state = retention(
        queries, keys_in, values_in, log_decay.reshape(1, rows)
    )
    states = exchange(state, NEAR)
    joined = joined_state(states)
    joined = exchange(joined, "zh")
    zh = lax.axis_index("zh").astype(jnp.int32).reshape(1)
    entering = incoming_state(zh, joined, states)
    entering = exchange(entering, NEAR)
    entering = entering.reshape(head_dim, head_dim)
    sent = mix(within, carry_q, entering, gate_in, head_gain.reshape(1, -1))
    mixed = exchange(sent.reshape(16, *sent.shape[2:]), GROUP + ("c",))
    here = jnp.stack([lax.axis_index(a).astype(jnp.int32) for a in ("x", "c", "y0")])
    normed, residual = group_rows(
        here, mixed.reshape(2, 8, *mixed.shape[1:]), near_w, far_w, near_s, far_s, norm_gain.reshape(1, -1)
    )
    y1 = lax.axis_index("y1").astype(jnp.int32).reshape(1)
    down_terms = feed_forward(y1, normed, weights)
    terms = exchange(down_terms.reshape(8, rows // 8, width), GROUP)
    result = residual
    for n in range(8):
        result = result + terms[n].astype(F32)
    return result.astype(BF16)


def solution(mesh):
    finer = Mesh(mesh.devices.reshape(*SIZES.values()), tuple(SIZES))
    return jax.shard_map(
        layer,
        mesh=finer,
        in_specs=(
            P(SP + TP, None),
            P(SP, TP),
            P(SP, TP),
            P(SP, TP),
            P(SP, TP),
            P(SP, TP),
            P(TP),
            P(TP, None),
            P(),
            P(SP, TP),
            P(SP, TP),
            P(TP, SP),
        ),
        out_specs=P(SP + TP, None),
        check_vma=False,
    )
```

```python
import jax
import jax.numpy as jnp
from jax import lax
from jax.experimental import pallas as pl
from jax.experimental.pallas import tpu as pltpu
from jax.sharding import Mesh
from jax.sharding import PartitionSpec as P


Z, Y = ("zh", "zl"), ("y1", "y0")
NEAR = ("zl",) + Y
SP = Z + Y
TP = ("x", "c")
GROUP = ("y0", "x")
SIZES = {"zh": 4, "zl": 4, "y1": 2, "y0": 2, "x": 4, "c": 2}
EPS = 1e-6
NEIGHBOURS = 16
F32, BF16 = jnp.float32, jnp.bfloat16


def vmem(count):
    return [pl.BlockSpec(memory_space=pltpu.VMEM)] * count


def kernel_cost(flops, moved, exps=0):
    return pl.CostEstimate(flops=flops, bytes_accessed=moved, transcendentals=exps)


def dot(a, b):
    return jnp.dot(a, b, preferred_element_type=F32)


def dot_nt(a, b):
    return lax.dot_general(a, b, (((1,), (1,)), ((), ())), preferred_element_type=F32)


def dot_tn(a, b):
    return lax.dot_general(a, b, (((0,), (0,)), ((), ())), preferred_element_type=F32)


def packed_state(state, total):
    width = state.shape[1]
    total = jnp.broadcast_to(total, (8, width))
    high = total.astype(BF16).astype(F32)
    mid = (total - high).astype(BF16).astype(F32)
    line = lax.broadcasted_iota(jnp.int32, total.shape, 0)
    terms = jnp.where(line == 0, high, jnp.where(line == 1, mid, total - high - mid))
    return jnp.concatenate([state, terms], axis=0).astype(BF16)


def unpacked_state(packed):
    part = packed.shape[0] - 8
    wide = packed.astype(F32)
    total = wide[part : part + 1] + wide[part + 1 : part + 2] + wide[part + 2 : part + 3]
    return wide[:part], total


def retention_kernel(q_ref, k_ref, v_ref, decay_ref, within_ref, carry_q_ref, state_ref):
    rows, head_dim = q_ref.shape
    scale = head_dim**-0.5
    at = lax.broadcasted_iota(jnp.int32, (rows, rows), 0)
    to = lax.broadcasted_iota(jnp.int32, (rows, rows), 1)
    causal = at >= to
    running = jnp.sum(jnp.where(causal, decay_ref[...], 0.0), axis=1, keepdims=True)
    across = jnp.sum(jnp.where(at == to, running, 0.0), axis=0, keepdims=True)
    total = running[rows - 1 : rows, :]
    q, k, v = q_ref[...], k_ref[...], v_ref[...]
    table = jnp.where(causal, jnp.exp(jnp.minimum(running - across, 0.0)), 0.0)
    scores = dot_nt(q, k) * scale
    within_ref[...] = dot((scores * table).astype(BF16), v)
    carry_q_ref[...] = (q.astype(F32) * jnp.exp(running)).astype(BF16)
    key_wide = (k.astype(F32) * scale * jnp.exp(total - running)).astype(BF16)
    state = dot_tn(key_wide, v)
    slices = state_ref.shape[0]
    part = head_dim // slices
    for n in range(slices):
        state_ref[n] = packed_state(state[n * part : (n + 1) * part], total)


def retention(q, k, v, decay):
    rows, head_dim = q.shape
    part = head_dim // NEIGHBOURS
    return pl.pallas_call(
        retention_kernel,
        out_shape=(
            jax.ShapeDtypeStruct((rows, head_dim), F32),
            jax.ShapeDtypeStruct((rows, head_dim), BF16),
            jax.ShapeDtypeStruct((NEIGHBOURS, part + 8, head_dim), BF16),
        ),
        in_specs=vmem(4),
        out_specs=vmem(3),
        cost_estimate=kernel_cost(6 * rows * rows * head_dim, 2**20, rows * rows),
        name="retention",
    )(q, k, v, decay)


def joined_kernel(states_ref, out_ref):
    state, total = unpacked_state(states_ref[0])
    for n in range(1, states_ref.shape[0]):
        own, decay = unpacked_state(states_ref[n])
        state = jnp.exp(decay) * state + own
        total = total + decay
    packed = packed_state(state, total)
    for n in range(out_ref.shape[0]):
        out_ref[n] = packed


def joined_state(states):
    _, lines, width = states.shape
    return pl.pallas_call(
        joined_kernel,
        out_shape=jax.ShapeDtypeStruct((SIZES["zh"], lines, width), BF16),
        in_specs=vmem(1),
        out_specs=pl.BlockSpec(memory_space=pltpu.VMEM),
        cost_estimate=kernel_cost(2**18, 2**18, 2**10),
        compiler_params=pltpu.CompilerParams(vmem_limit_bytes=2 * 2**20),
        name="joined_state",
    )(states)


def incoming_kernel(here_ref, joined_ref, states_ref, out_ref):
    here = here_ref[0]
    carried = jnp.zeros(out_ref.shape[1:], F32)
    for n in range(joined_ref.shape[0]):
        own, decay = unpacked_state(joined_ref[n])
        carried = jnp.where(n < here, jnp.exp(decay) * carried + own, carried)
    for n in range(out_ref.shape[0]):
        out_ref[n] = carried.astype(BF16)
        own, decay = unpacked_state(states_ref[n])
        carried = jnp.exp(decay) * carried + own


def incoming_state(here, joined, states):
    count, lines, width = states.shape
    return pl.pallas_call(
        incoming_kernel,
        out_shape=jax.ShapeDtypeStruct((count, lines - 8, width), BF16),
        in_specs=[pl.BlockSpec(memory_space=pltpu.SMEM)] + vmem(2),
        out_specs=pl.BlockSpec(memory_space=pltpu.VMEM),
        cost_estimate=kernel_cost(2**19, 2**19, 2**12),
        compiler_params=pltpu.CompilerParams(vmem_limit_bytes=2 * 2**20),
        name="incoming_state",
    )(here, joined, states)


def mix_kernel(within_ref, carry_q_ref, state_ref, gate_ref, gain_ref, out_ref):
    retained = within_ref[...] + dot(carry_q_ref[...], state_ref[...])
    center = jnp.mean(retained, axis=-1, keepdims=True)
    off = retained - center
    spread = jnp.mean(off * off, axis=-1, keepdims=True)
    normed = off * lax.rsqrt(spread + EPS) * gain_ref[...].astype(F32)
    gate = gate_ref[...].astype(F32)
    mixed = (gate * jax.nn.sigmoid(gate) * normed).astype(BF16)
    places, cores, blocks, lines, _ = out_ref.shape
    for core in range(cores):
        for n in range(blocks):
            first = (n * cores + core) * lines
            piece = mixed[first : first + lines]
            for place in range(places):
                out_ref[place, core, n] = piece


def mix(within, carry_q, state, gate, gain):
    rows, width = within.shape
    return pl.pallas_call(
        mix_kernel,
        out_shape=jax.ShapeDtypeStruct((8, 2, 4, rows // 8, width), BF16),
        in_specs=vmem(5),
        out_specs=pl.BlockSpec(memory_space=pltpu.VMEM),
        cost_estimate=kernel_cost(2 * rows * width * width, 2**20, rows * width),
        name="mix",
    )(within, carry_q, state, gate, gain)


def rows_kernel(
    here_ref, mixed_ref, near_w_ref, far_w_ref, near_s_ref, far_s_ref, gain_ref, normed_ref, own_ref, residual, normed, sems
):
    halves, _, blocks, lines, head_dim = mixed_ref.shape
    count, width = normed_ref.shape
    x, c, y0 = here_ref[0], here_ref[1], here_ref[2]

    def heads_of(core):
        return jnp.concatenate(
            [
                jnp.concatenate(
                    [mixed_ref[n, ((x + 4 - r) % 4) * 2 + core].reshape(count // halves, head_dim) for r in range(4)],
                    axis=1,
                )
                for n in range(halves)
            ],
            axis=0,
        )

    near, far = heads_of(c), heads_of(1 - c)
    step = width // 4
    squares = jnp.zeros((count, 1), F32)
    for n in range(4):
        span = slice(n * step, (n + 1) * step)
        rows = []
        for half in range(halves):
            for block in range(blocks):
                at = (x + 4 - block) % 4
                rows.append(jnp.where(y0 == half, near_s_ref[at, :, span], far_s_ref[at, :, span]))
        part = (
            jnp.concatenate(rows, axis=0).astype(F32)
            + dot(near, near_w_ref[:, span])
            + dot(far, far_w_ref[:, span])
        )
        residual[:, span] = part
        squares += jnp.sum(part * part, axis=-1, keepdims=True)
    factor = lax.rsqrt(squares / width + EPS)
    copies = []
    for n in range(4):
        span = slice(n * step, (n + 1) * step)
        normed[:, span] = (residual[:, span] * factor * gain_ref[:, span].astype(F32)).astype(BF16)
        copies.append(pltpu.make_async_copy(normed.at[:, span], normed_ref.at[:, span], sems.at[n]))
        copies[n].start()
    first = pl.multiple_of((y0 * blocks + x) * lines, lines)
    own_ref[...] = residual[pl.ds(first, lines), :]
    for copy in copies:
        copy.wait()


def group_rows(here, mixed, near_w, far_w, near_s, far_s, gain):
    lines, width = near_s.shape[1:]
    count = 8 * lines
    return pl.pallas_call(
        rows_kernel,
        out_shape=(
            jax.ShapeDtypeStruct((count, width), BF16),
            jax.ShapeDtypeStruct((lines, width), F32),
        ),
        in_specs=[pl.BlockSpec(memory_space=pltpu.SMEM)] + vmem(6),
        out_specs=[pl.BlockSpec(memory_space=pltpu.HBM)] + vmem(1),
        scratch_shapes=[
            pltpu.VMEM((count, width), F32),
            pltpu.VMEM((count, width), BF16),
            pltpu.SemaphoreType.DMA((4,)),
        ],
        cost_estimate=kernel_cost(2 * count * width * 1024, 2**23),
        compiler_params=pltpu.CompilerParams(vmem_limit_bytes=20 * 2**20),
        name="group_rows",
    )(here, mixed, near_w, far_w, near_s, far_s, gain)


CHUNKS = (2, 1, 1)
AHEAD = 2


def ffn_kernel(rows_ref, weight_ref, out_ref, rows, held, rows_sem, sems):
    z, _, _, kinds, lines, hidden_width = weight_ref.shape

    def copies(kind, n):
        each = z // CHUNKS[kind]
        span = pl.ds(n * each, each)
        return [
            pltpu.make_async_copy(
                weight_ref.at[span, y0, y1, kind],
                held.at[kind, span, y1, y0],
                sems.at[kind, n, 2 * y1 + y0],
            )
            for y1 in range(2)
            for y0 in range(2)
        ]

    order = [(kind, n) for kind in range(kinds) for n in range(CHUNKS[kind])]

    def start(at):
        for place in order[at : at + 1]:
            for copy in copies(*place):
                copy.start()

    def arrived(kind, n):
        each = z // CHUNKS[kind]
        for copy in copies(kind, n):
            copy.wait()
        start(order.index((kind, n)) + AHEAD)
        depth = each * 4 * lines
        return held[kind, n * each : (n + 1) * each].reshape(depth, hidden_width), depth

    fetch = pltpu.make_async_copy(rows_ref, rows, rows_sem)
    fetch.start()
    for at in range(AHEAD):
        start(at)
    fetch.wait()
    sums = []
    for kind in (0, 1):
        total = None
        for n in range(CHUNKS[kind]):
            block, depth = arrived(kind, n)
            part = dot(rows[:, n * depth : (n + 1) * depth], block)
            total = part if total is None else total + part
        sums.append(total)
    gate_sum, up_sum = sums
    hidden = (gate_sum * jax.nn.sigmoid(gate_sum) * up_sum).astype(BF16)
    for n in range(CHUNKS[2]):
        block, depth = arrived(2, n)
        out_ref[:, n * depth : (n + 1) * depth] = dot_nt(hidden, block).astype(BF16)


def feed_forward(rows, weights):
    count, width = rows.shape
    z, y0, y1, kinds, lines, hidden_width = weights.shape
    return pl.pallas_call(
        ffn_kernel,
        out_shape=jax.ShapeDtypeStruct((count, width), BF16),
        in_specs=[pl.BlockSpec(memory_space=pltpu.HBM)] * 2,
        out_specs=pl.BlockSpec(memory_space=pltpu.VMEM),
        scratch_shapes=[
            pltpu.VMEM((count, width), BF16),
            pltpu.VMEM((kinds, z, y1, y0, lines, hidden_width), BF16),
            pltpu.SemaphoreType.DMA,
            pltpu.SemaphoreType.DMA((kinds, max(CHUNKS), 4)),
        ],
        cost_estimate=kernel_cost(6 * count * width * hidden_width, 2**23, count * hidden_width),
        compiler_params=pltpu.CompilerParams(vmem_limit_bytes=52 * 2**20),
        name="feed_forward",
    )(rows, weights)


def moved(value, axes, place):
    lengths = [SIZES[a] for a in axes]
    pairs = []
    for y1 in range(lengths[0]):
        for y0 in range(lengths[1]):
            for c in range(lengths[2]):
                a, b, d = place(y1, y0, c)
                pairs.append(((y1 * 2 + y0) * 2 + c, (a * 2 + b) * 2 + d))
    return lax.ppermute(value, axes, pairs)


def shifted(value, axis, by):
    length = SIZES[axis]
    return lax.ppermute(value, axis, [(i, (i + by) % length) for i in range(length)])


def exchange(tiles, axes):
    return lax.all_to_all(tiles, axes, split_axis=0, concat_axis=0, tiled=True)


def gathered_weights(gate_weight, up_weight, down_weight):
    mine = jnp.concatenate([gate_weight, up_weight, down_weight.T], axis=0)
    lines, width = mine.shape
    axes = ("y1", "y0", "c")
    near = moved(mine, axes, lambda y1, y0, c: (y1, c, y0))
    far = moved(mine, axes, lambda y1, y0, c: (1 - y1, c, y0))
    upper = lax.axis_index("y1") == 1
    pair = jnp.stack([jnp.where(upper, far, near), jnp.where(upper, near, far)])
    whole = lax.all_gather(pair, Z + ("c",), axis=0)
    return whole.reshape(16, 2, 2, 3, lines // 3, width)


def layer(
    stream,
    queries,
    keys_in,
    values_in,
    gate_in,
    log_decay,
    head_gain,
    out_weight,
    norm_gain,
    gate_weight,
    up_weight,
    down_weight,
):
    weights = gathered_weights(gate_weight, up_weight, down_weight)
    rows, width = queries.shape[0], stream.shape[1]
    head_dim = queries.shape[1]
    found = [out_weight] + [shifted(out_weight, "x", r) for r in (1, 2, 3)]
    others = [shifted(stream, "x", r) for r in (1, 2, 3)]
    near_s = jnp.stack([stream, *others])
    far_s = shifted(near_s, "y0", 1)
    near_w = jnp.concatenate(found, axis=0)
    far_w = shifted(near_w, "c", 1)
    within, carry_q, state = retention(
        queries, keys_in, values_in, log_decay.reshape(1, rows)
    )
    states = exchange(state, NEAR)
    joined = joined_state(states)
    joined = exchange(joined, "zh")
    zh = lax.axis_index("zh").astype(jnp.int32).reshape(1)
    entering = incoming_state(zh, joined, states)
    entering = exchange(entering, NEAR)
    entering = entering.reshape(head_dim, head_dim)
    sent = mix(within, carry_q, entering, gate_in, head_gain.reshape(1, -1))
    mixed = exchange(sent.reshape(16, *sent.shape[2:]), GROUP + ("c",))
    here = jnp.stack([lax.axis_index(a).astype(jnp.int32) for a in ("x", "c", "y0")])
    normed, residual = group_rows(
        here, mixed.reshape(2, 8, *mixed.shape[1:]), near_w, far_w, near_s, far_s, norm_gain.reshape(1, -1)
    )
    down_terms = feed_forward(normed, weights)
    mixer_out = exchange(down_terms.reshape(8, rows // 8, width), GROUP).astype(F32).sum(axis=0)
    return (residual + mixer_out).astype(BF16)


def solution(mesh):
    finer = Mesh(mesh.devices.reshape(*SIZES.values()), tuple(SIZES))
    return jax.shard_map(
        layer,
        mesh=finer,
        in_specs=(
            P(SP + TP, None),
            P(SP, TP),
            P(SP, TP),
            P(SP, TP),
            P(SP, TP),
            P(SP, TP),
            P(TP),
            P(TP, None),
            P(),
            P(SP, TP),
            P(SP, TP),
            P(TP, SP),
        ),
        out_specs=P(SP + TP, None),
        check_vma=False,
    )
```

```python
import jax
import jax.numpy as jnp
from jax import lax
from jax.experimental import pallas as pl
from jax.experimental.pallas import tpu as pltpu
from jax.sharding import Mesh
from jax.sharding import PartitionSpec as P


Z, Y = ("zh", "zl"), ("y1", "y0")
NEAR = ("zl",) + Y
SP = Z + Y
TP = ("x", "c")
GROUP = ("y0", "x")
SIZES = {"zh": 4, "zl": 4, "y1": 2, "y0": 2, "x": 4, "c": 2}
EPS = 1e-6
NEIGHBOURS = 16
F32, BF16 = jnp.float32, jnp.bfloat16


def vmem(count):
    return [pl.BlockSpec(memory_space=pltpu.VMEM)] * count


def kernel_cost(flops, moved, exps=0):
    return pl.CostEstimate(flops=flops, bytes_accessed=moved, transcendentals=exps)


def dot(a, b):
    return jnp.dot(a, b, preferred_element_type=F32)


def dot_nt(a, b):
    return lax.dot_general(a, b, (((1,), (1,)), ((), ())), preferred_element_type=F32)


def dot_tn(a, b):
    return lax.dot_general(a, b, (((0,), (0,)), ((), ())), preferred_element_type=F32)


def packed_state(state, total):
    width = state.shape[1]
    total = jnp.broadcast_to(total, (8, width))
    high = total.astype(BF16).astype(F32)
    mid = (total - high).astype(BF16).astype(F32)
    line = lax.broadcasted_iota(jnp.int32, total.shape, 0)
    terms = jnp.where(line == 0, high, jnp.where(line == 1, mid, total - high - mid))
    return jnp.concatenate([state, terms], axis=0).astype(BF16)


def unpacked_state(packed):
    part = packed.shape[0] - 8
    wide = packed.astype(F32)
    total = wide[part : part + 1] + wide[part + 1 : part + 2] + wide[part + 2 : part + 3]
    return wide[:part], total


def retention_kernel(q_ref, k_ref, v_ref, decay_ref, within_ref, carry_q_ref, state_ref):
    rows, head_dim = q_ref.shape
    scale = head_dim**-0.5
    at = lax.broadcasted_iota(jnp.int32, (rows, rows), 0)
    to = lax.broadcasted_iota(jnp.int32, (rows, rows), 1)
    causal = at >= to
    running = jnp.sum(jnp.where(causal, decay_ref[...], 0.0), axis=1, keepdims=True)
    across = jnp.sum(jnp.where(at == to, running, 0.0), axis=0, keepdims=True)
    total = running[rows - 1 : rows, :]
    q, k, v = q_ref[...], k_ref[...], v_ref[...]
    table = jnp.where(causal, jnp.exp(jnp.minimum(running - across, 0.0)), 0.0)
    scores = dot_nt(q, k) * scale
    within_ref[...] = dot((scores * table).astype(BF16), v)
    carry_q_ref[...] = (q.astype(F32) * jnp.exp(running)).astype(BF16)
    key_wide = (k.astype(F32) * scale * jnp.exp(total - running)).astype(BF16)
    state = dot_tn(key_wide, v)
    slices = state_ref.shape[0]
    part = head_dim // slices
    for n in range(slices):
        state_ref[n] = packed_state(state[n * part : (n + 1) * part], total)


def retention(q, k, v, decay):
    rows, head_dim = q.shape
    part = head_dim // NEIGHBOURS
    return pl.pallas_call(
        retention_kernel,
        out_shape=(
            jax.ShapeDtypeStruct((rows, head_dim), F32),
            jax.ShapeDtypeStruct((rows, head_dim), BF16),
            jax.ShapeDtypeStruct((NEIGHBOURS, part + 8, head_dim), BF16),
        ),
        in_specs=vmem(4),
        out_specs=vmem(3),
        cost_estimate=kernel_cost(6 * rows * rows * head_dim, 2**20, rows * rows),
        name="retention",
    )(q, k, v, decay)


def joined_kernel(states_ref, out_ref):
    state, total = unpacked_state(states_ref[0])
    for n in range(1, states_ref.shape[0]):
        own, decay = unpacked_state(states_ref[n])
        state = jnp.exp(decay) * state + own
        total = total + decay
    packed = packed_state(state, total)
    for n in range(out_ref.shape[0]):
        out_ref[n] = packed


def joined_state(states):
    _, lines, width = states.shape
    return pl.pallas_call(
        joined_kernel,
        out_shape=jax.ShapeDtypeStruct((SIZES["zh"], lines, width), BF16),
        in_specs=vmem(1),
        out_specs=pl.BlockSpec(memory_space=pltpu.VMEM),
        cost_estimate=kernel_cost(2**18, 2**18, 2**10),
        compiler_params=pltpu.CompilerParams(vmem_limit_bytes=2 * 2**20),
        name="joined_state",
    )(states)


def incoming_kernel(here_ref, joined_ref, states_ref, out_ref):
    here = here_ref[0]
    carried = jnp.zeros(out_ref.shape[1:], F32)
    for n in range(joined_ref.shape[0]):
        own, decay = unpacked_state(joined_ref[n])
        carried = jnp.where(n < here, jnp.exp(decay) * carried + own, carried)
    for n in range(out_ref.shape[0]):
        out_ref[n] = carried.astype(BF16)
        own, decay = unpacked_state(states_ref[n])
        carried = jnp.exp(decay) * carried + own


def incoming_state(here, joined, states):
    count, lines, width = states.shape
    return pl.pallas_call(
        incoming_kernel,
        out_shape=jax.ShapeDtypeStruct((count, lines - 8, width), BF16),
        in_specs=[pl.BlockSpec(memory_space=pltpu.SMEM)] + vmem(2),
        out_specs=pl.BlockSpec(memory_space=pltpu.VMEM),
        cost_estimate=kernel_cost(2**19, 2**19, 2**12),
        compiler_params=pltpu.CompilerParams(vmem_limit_bytes=2 * 2**20),
        name="incoming_state",
    )(here, joined, states)


def mix_kernel(within_ref, carry_q_ref, state_ref, gate_ref, gain_ref, out_ref):
    retained = within_ref[...] + dot(carry_q_ref[...], state_ref[...])
    center = jnp.mean(retained, axis=-1, keepdims=True)
    off = retained - center
    spread = jnp.mean(off * off, axis=-1, keepdims=True)
    normed = off * lax.rsqrt(spread + EPS) * gain_ref[...].astype(F32)
    gate = gate_ref[...].astype(F32)
    mixed = (gate * jax.nn.sigmoid(gate) * normed).astype(BF16)
    places, cores, blocks, lines, _ = out_ref.shape
    for core in range(cores):
        for n in range(blocks):
            first = (n * cores + core) * lines
            piece = mixed[first : first + lines]
            for place in range(places):
                out_ref[place, core, n] = piece


def mix(within, carry_q, state, gate, gain):
    rows, width = within.shape
    return pl.pallas_call(
        mix_kernel,
        out_shape=jax.ShapeDtypeStruct((8, 2, 4, rows // 8, width), BF16),
        in_specs=vmem(5),
        out_specs=pl.BlockSpec(memory_space=pltpu.VMEM),
        cost_estimate=kernel_cost(2 * rows * width * width, 2**20, rows * width),
        name="mix",
    )(within, carry_q, state, gate, gain)


def rows_kernel(
    here_ref, mixed_ref, near_w_ref, far_w_ref, near_s_ref, far_s_ref, gain_ref, normed_ref, own_ref, residual, normed, sems
):
    halves, _, blocks, lines, head_dim = mixed_ref.shape
    count, width = normed_ref.shape
    x, c, y0 = here_ref[0], here_ref[1], here_ref[2]

    def heads_of(core):
        return jnp.concatenate(
            [
                jnp.concatenate(
                    [mixed_ref[n, ((x + 4 - r) % 4) * 2 + core].reshape(count // halves, head_dim) for r in range(4)],
                    axis=1,
                )
                for n in range(halves)
            ],
            axis=0,
        )

    near, far = heads_of(c), heads_of(1 - c)
    step = width // 4
    squares = jnp.zeros((count, 1), F32)
    for n in range(4):
        span = slice(n * step, (n + 1) * step)
        rows = []
        for half in range(halves):
            for block in range(blocks):
                at = (x + 4 - block) % 4
                rows.append(jnp.where(y0 == half, near_s_ref[at, :, span], far_s_ref[at, :, span]))
        part = (
            jnp.concatenate(rows, axis=0).astype(F32)
            + dot(near, near_w_ref[:, span])
            + dot(far, far_w_ref[:, span])
        )
        residual[:, span] = part
        squares += jnp.sum(part * part, axis=-1, keepdims=True)
    factor = lax.rsqrt(squares / width + EPS)
    copies = []
    for n in range(4):
        span = slice(n * step, (n + 1) * step)
        normed[:, span] = (residual[:, span] * factor * gain_ref[:, span].astype(F32)).astype(BF16)
        copies.append(pltpu.make_async_copy(normed.at[:, span], normed_ref.at[:, span], sems.at[n]))
        copies[n].start()
    first = pl.multiple_of((y0 * blocks + x) * lines, lines)
    own_ref[...] = residual[pl.ds(first, lines), :]
    for copy in copies:
        copy.wait()


def group_rows(here, mixed, near_w, far_w, near_s, far_s, gain):
    lines, width = near_s.shape[1:]
    count = 8 * lines
    return pl.pallas_call(
        rows_kernel,
        out_shape=(
            jax.ShapeDtypeStruct((count, width), BF16),
            jax.ShapeDtypeStruct((lines, width), F32),
        ),
        in_specs=[pl.BlockSpec(memory_space=pltpu.SMEM)] + vmem(6),
        out_specs=[pl.BlockSpec(memory_space=pltpu.HBM)] + vmem(1),
        scratch_shapes=[
            pltpu.VMEM((count, width), F32),
            pltpu.VMEM((count, width), BF16),
            pltpu.SemaphoreType.DMA((4,)),
        ],
        cost_estimate=kernel_cost(2 * count * width * 1024, 2**23),
        compiler_params=pltpu.CompilerParams(vmem_limit_bytes=20 * 2**20),
        name="group_rows",
    )(here, mixed, near_w, far_w, near_s, far_s, gain)


CHUNKS = (2, 1, 1)
AHEAD = 2


def ffn_kernel(rows_ref, weight_ref, out_ref, rows, held, rows_sem, sems):
    z, _, _, kinds, lines, hidden_width = weight_ref.shape

    def copies(kind, n):
        each = z // CHUNKS[kind]
        span = pl.ds(n * each, each)
        return [
            pltpu.make_async_copy(
                weight_ref.at[span, y0, y1, kind],
                held.at[kind, span, y1, y0],
                sems.at[kind, n, 2 * y1 + y0],
            )
            for y1 in range(2)
            for y0 in range(2)
        ]

    order = [(kind, n) for kind in range(kinds) for n in range(CHUNKS[kind])]

    def start(at):
        for place in order[at : at + 1]:
            for copy in copies(*place):
                copy.start()

    def arrived(kind, n):
        each = z // CHUNKS[kind]
        for copy in copies(kind, n):
            copy.wait()
        start(order.index((kind, n)) + AHEAD)
        depth = each * 4 * lines
        return held[kind, n * each : (n + 1) * each].reshape(depth, hidden_width), depth

    fetch = pltpu.make_async_copy(rows_ref, rows, rows_sem)
    start(0)
    fetch.start()
    for at in range(1, AHEAD):
        start(at)
    fetch.wait()
    sums = []
    for kind in (0, 1):
        total = None
        for n in range(CHUNKS[kind]):
            block, depth = arrived(kind, n)
            part = dot(rows[:, n * depth : (n + 1) * depth], block)
            total = part if total is None else total + part
        sums.append(total)
    gate_sum, up_sum = sums
    hidden = (gate_sum * jax.nn.sigmoid(gate_sum) * up_sum).astype(BF16)
    for n in range(CHUNKS[2]):
        block, depth = arrived(2, n)
        out_ref[:, n * depth : (n + 1) * depth] = dot_nt(hidden, block).astype(BF16)


def feed_forward(rows, weights):
    count, width = rows.shape
    z, y0, y1, kinds, lines, hidden_width = weights.shape
    return pl.pallas_call(
        ffn_kernel,
        out_shape=jax.ShapeDtypeStruct((count, width), BF16),
        in_specs=[pl.BlockSpec(memory_space=pltpu.HBM)] * 2,
        out_specs=pl.BlockSpec(memory_space=pltpu.VMEM),
        scratch_shapes=[
            pltpu.VMEM((count, width), BF16),
            pltpu.VMEM((kinds, z, y1, y0, lines, hidden_width), BF16),
            pltpu.SemaphoreType.DMA,
            pltpu.SemaphoreType.DMA((kinds, max(CHUNKS), 4)),
        ],
        cost_estimate=kernel_cost(6 * count * width * hidden_width, 2**23, count * hidden_width),
        compiler_params=pltpu.CompilerParams(vmem_limit_bytes=52 * 2**20),
        name="feed_forward",
    )(rows, weights)


def moved(value, axes, place):
    lengths = [SIZES[a] for a in axes]
    pairs = []
    for y1 in range(lengths[0]):
        for y0 in range(lengths[1]):
            for c in range(lengths[2]):
                a, b, d = place(y1, y0, c)
                pairs.append(((y1 * 2 + y0) * 2 + c, (a * 2 + b) * 2 + d))
    return lax.ppermute(value, axes, pairs)


def shifted(value, axis, by):
    length = SIZES[axis]
    return lax.ppermute(value, axis, [(i, (i + by) % length) for i in range(length)])


def exchange(tiles, axes):
    return lax.all_to_all(tiles, axes, split_axis=0, concat_axis=0, tiled=True)


def gathered_weights(gate_weight, up_weight, down_weight):
    mine = jnp.concatenate([gate_weight, up_weight, down_weight.T], axis=0)
    lines, width = mine.shape
    axes = ("y1", "y0", "c")
    near = moved(mine, axes, lambda y1, y0, c: (y1, c, y0))
    far = moved(mine, axes, lambda y1, y0, c: (1 - y1, c, y0))
    upper = lax.axis_index("y1") == 1
    pair = jnp.stack([jnp.where(upper, far, near), jnp.where(upper, near, far)])
    whole = lax.all_gather(pair, Z + ("c",), axis=0)
    return whole.reshape(16, 2, 2, 3, lines // 3, width)


def layer(
    stream,
    queries,
    keys_in,
    values_in,
    gate_in,
    log_decay,
    head_gain,
    out_weight,
    norm_gain,
    gate_weight,
    up_weight,
    down_weight,
):
    weights = gathered_weights(gate_weight, up_weight, down_weight)
    rows, width = queries.shape[0], stream.shape[1]
    head_dim = queries.shape[1]
    found = [out_weight] + [shifted(out_weight, "x", r) for r in (1, 2, 3)]
    others = [shifted(stream, "x", r) for r in (1, 2, 3)]
    near_s = jnp.stack([stream, *others])
    far_s = shifted(near_s, "y0", 1)
    near_w = jnp.concatenate(found, axis=0)
    far_w = shifted(near_w, "c", 1)
    within, carry_q, state = retention(
        queries, keys_in, values_in, log_decay.reshape(1, rows)
    )
    states = exchange(state, NEAR)
    joined = joined_state(states)
    joined = exchange(joined, "zh")
    zh = lax.axis_index("zh").astype(jnp.int32).reshape(1)
    entering = incoming_state(zh, joined, states)
    entering = exchange(entering, NEAR)
    entering = entering.reshape(head_dim, head_dim)
    sent = mix(within, carry_q, entering, gate_in, head_gain.reshape(1, -1))
    mixed = exchange(sent.reshape(16, *sent.shape[2:]), GROUP + ("c",))
    here = jnp.stack([lax.axis_index(a).astype(jnp.int32) for a in ("x", "c", "y0")])
    normed, residual = group_rows(
        here, mixed.reshape(2, 8, *mixed.shape[1:]), near_w, far_w, near_s, far_s, norm_gain.reshape(1, -1)
    )
    down_terms = feed_forward(normed, weights)
    terms = exchange(down_terms.reshape(8, rows // 8, width), GROUP)
    result = residual
    for n in range(8):
        result = result + terms[n].astype(F32)
    return result.astype(BF16)


def solution(mesh):
    finer = Mesh(mesh.devices.reshape(*SIZES.values()), tuple(SIZES))
    return jax.shard_map(
        layer,
        mesh=finer,
        in_specs=(
            P(SP + TP, None),
            P(SP, TP),
            P(SP, TP),
            P(SP, TP),
            P(SP, TP),
            P(SP, TP),
            P(TP),
            P(TP, None),
            P(),
            P(SP, TP),
            P(SP, TP),
            P(TP, SP),
        ),
        out_specs=P(SP + TP, None),
        check_vma=False,
    )
```
